512 devices in a mesh: kv: 64 (over z, y), tp: 8 (over x, core).
Axes of the slice: x: 4, y: 4, z: 16, core: 2. Of those that a mesh axis runs over, the one named last changes fastest.
Arguments:
- tokens: bfloat16 [4, 4, 4096], replicated, may hold values from -6 to 6
- parents: int32 [4, 4], replicated, may hold values from -1 to 2, as said below
- lengths: int32 [4], replicated, may hold values from 1 to 8184, as said below
- accepted: int32 [4], replicated, may hold values from 0 to 4
- in_gain: float32 [4096], replicated, may hold values from 0.1 to 1.9
- w_query: bfloat16 [4096, 3072], P('kv', 'tp'), may hold values from -0.09375 to 0.09375
- w_latent: bfloat16 [4096, 1024], P('kv'), may hold values from -0.09375 to 0.09375
- w_rope_key: bfloat16 [4096, 32], replicated, may hold values from -0.09375 to 0.09375
- latent_gain: float32 [1024], replicated, may hold values from 0.1 to 1.9
- query_gain: float32 [96], replicated, may hold values from 0.4 to 160, as said below
- key_gain: float32 [96], replicated, may hold values from 0.1 to 1.9
- w_key_up: bfloat16 [1024, 2048], P(None, 'tp'), may hold values from -0.1875 to 0.1875
- w_value_up: bfloat16 [1024, 2048], P(None, 'tp'), may hold values from -0.1875 to 0.1875
- w_out: bfloat16 [2048, 4096], P('tp', 'kv'), may hold values from -1 to 1
- out_gain: float32 [4096], P('kv'), may hold values from 0.1 to 1.9
- cache_latent: bfloat16 [4, 8192, 1024], P(None, 'kv'), may hold values from -6 to 6
- cache_rope: bfloat16 [4, 8192, 32], P(None, 'kv'), may hold values from -6 to 6
Outputs:
- mixed: bfloat16 [4, 4, 4096], P(None, None, 'kv')
- new_latent: bfloat16 [4, 8192, 1024], P(None, 'kv')
- new_rope: bfloat16 [4, 8192, 32], P(None, 'kv')
The draws below stay inside these ranges and needn't reach their ends.
Inputs may be any that keep to these rules, and one draw needn't show every extreme that they name: parents[s, 0] is -1; for i of 1 or more parents[s, i] lies in 0 to i - 1. `lengths`: the first sequence's length is at most 8, the last one's at least 8056. `query_gain`: positive.
All inputs are finite; a program needn't handle non-finite values.
Results may differ from the reference program's by a relative error of at most 0.008.
The reference program's roundings to bfloat16 on the way count: a program that leaves them out, or rounds other values in their place, can miss the bound.
Values sent between devices are 32-bit elements; how exact they have to be, the bound alone decides.
No kernel may reach another device: no remote copies, remote signals or barrier semaphores. Data moves between devices by JAX's collectives and lax.ppermute only.
A program may use at most 64 MiB of HBM per device.

```python
import jax
import jax.numpy as jnp
from jax import lax

D = 4096
HEADS = 32
NOPE = 64
ROPE = 32
QK = 96
VDIM = 64
LATENT = 1024
SEQS = 4
PROPS = 4
POS_DEV = 128
CACHE_LEN = 8192


def draw_parents(key, part):
    raw_bits = jax.random.randint(jax.random.fold_in(key, 11), (SEQS, PROPS), 0, 1 << 20)
    indices = jnp.arange(PROPS, dtype=jnp.int32)
    chosen = raw_bits % jnp.maximum(indices, 1)[None, :]
    return jnp.where(indices[None, :] == 0, -1, chosen).astype(jnp.int32)


def draw_lengths(key, part):
    key_short, key_edge, key_backward, key_last = jax.random.split(jax.random.fold_in(key, 23), 4)
    short_len = jax.random.randint(key_short, (1,), 1, 2 * PROPS + 1)
    blocks = jax.random.randint(key_edge, (SEQS - 2,), 1, CACHE_LEN // POS_DEV)
    backward = jax.random.randint(key_backward, (SEQS - 2,), 1, PROPS + 1)
    middle = blocks * POS_DEV - backward
    last_len = jax.random.randint(key_last, (1,), CACHE_LEN - POS_DEV - 2 * PROPS, CACHE_LEN - 2 * PROPS + 1)
    return jnp.concatenate([short_len, middle, last_len]).astype(jnp.int32)


def draw_query_gain(key, part):
    key_noise = jax.random.fold_in(jax.random.fold_in(key, 37), 0)
    key_pick = jax.random.fold_in(jax.random.fold_in(key, 37), 2)
    order = jax.random.permutation(key_pick, NOPE)
    dims = jnp.arange(QK, dtype=jnp.int32)
    strong = (dims == order[0]) | (dims == order[1])
    noise = jax.random.normal(key_noise, (QK,), jnp.float32)
    base = jnp.exp(0.3 * jnp.clip(noise, -3.0, 3.0))
    return jnp.where(strong, 100.0, base).astype(jnp.float32)


def draw_w_out(key, part):
    key_entries, key_columns = jax.random.split(jax.random.fold_in(key, 41))
    fraction = jnp.arange(D, dtype=jnp.float32) / D
    jitter = jnp.exp(jax.random.uniform(key_columns, (D,), jnp.float32, -0.7, 0.7))
    entries = jnp.clip(jax.random.normal(key_entries, (HEADS * VDIM, D), jnp.float32), -5.0, 5.0)
    column_scale = 10.0 ** (fraction - 0.5) * jitter
    return (entries * column_scale[None, :] * (HEADS * VDIM) ** (-0.5)).astype(jnp.bfloat16)


def touch_ends(drawn, key, least, top_value):
    longest = drawn.shape.index(max(drawn.shape))
    spots = []
    for shift in (0, 1):
        where = [jax.random.randint(jax.random.fold_in(key, axis), (), 0, length) for axis, length in enumerate(drawn.shape)]
        where[longest] = (where[longest] + shift) % drawn.shape[longest]
        spots.append(tuple(where))
    return drawn.at[spots[0]].set(least).at[spots[1]].set(top_value)


def levels(stream_key, shape, cuts, low, top_value):
    factor_of = 1.0
    for dim, parts in cuts:
        steps = jax.random.uniform(jax.random.fold_in(jax.random.fold_in(stream_key, 6), dim), (parts,), jnp.float32, low / len(cuts), top_value / len(cuts))
        factor_of = factor_of * jnp.repeat(jnp.exp(steps), shape[dim] // parts).reshape((-1,) + (1,) * (len(shape) - 1 - dim))
    return factor_of


def normal_values(stream_key, shape, scale, reach, pieces=(), kind=jnp.bfloat16):
    gain = levels(stream_key, shape, pieces, -0.22, 0.18) if pieces else 1.0
    values = jax.random.normal(stream_key, shape, jnp.float32) * scale * gain
    return jnp.minimum(jnp.maximum(values, -reach), reach).astype(kind)


def setup_inputs(seed: int = 0) -> dict:
    streams_of = jax.random.split(jax.random.key(seed), 18)
    return {
        "tokens": normal_values(streams_of[0], (SEQS, PROPS, D), 1.0, 6.0),
        "parents": draw_parents(jax.random.fold_in(streams_of[17], 71), 0),
        "lengths": draw_lengths(jax.random.fold_in(streams_of[17], 71), 0),
        "accepted": touch_ends(jax.random.randint(streams_of[3], (SEQS,), 0, PROPS + 1), jax.random.fold_in(streams_of[3], 1), 0, PROPS).astype(jnp.int32),
        "in_gain": jnp.clip(1.0 + 0.18 * jax.random.normal(streams_of[4], (D,), jnp.float32), 0.1, 1.9),
        "w_query": normal_values(streams_of[5], (D, HEADS * QK), D ** -0.5, 0.09375, ((0, 64), (1, 8))),
        "w_latent": normal_values(streams_of[6], (D, LATENT), D ** -0.5, 0.09375, ((0, 64),)),
        "w_rope_key": normal_values(streams_of[7], (D, ROPE), D ** -0.5, 0.09375),
        "latent_gain": jnp.clip(1.0 + 0.18 * jax.random.normal(streams_of[8], (LATENT,), jnp.float32), 0.1, 1.9),
        "query_gain": draw_query_gain(jax.random.fold_in(streams_of[17], 71), 0),
        "key_gain": jnp.clip(1.0 + 0.18 * jax.random.normal(streams_of[10], (QK,), jnp.float32), 0.1, 1.9),
        "w_key_up": normal_values(streams_of[11], (LATENT, HEADS * NOPE), LATENT ** -0.5, 0.1875, ((1, 8),)),
        "w_value_up": normal_values(streams_of[12], (LATENT, HEADS * VDIM), LATENT ** -0.5, 0.1875, ((1, 8),)),
        "w_out": draw_w_out(jax.random.fold_in(streams_of[17], 71), 0),
        "out_gain": jnp.clip(1.0 + 0.18 * jax.random.normal(streams_of[14], (D,), jnp.float32), 0.1, 1.9),
        "cache_latent": normal_values(streams_of[15], (SEQS, CACHE_LEN, LATENT), 1.0, 6.0, ((1, 64),)),
        "cache_rope": normal_values(streams_of[16], (SEQS, CACHE_LEN, ROPE), 1.0, 6.0, ((1, 64),)),
    }


epsilon = 1e-06
rope_base = 10000.0

def ancestry(parents):
    prop_count = parents.shape[-1]
    indices = jnp.arange(prop_count, dtype=jnp.int32)
    step_map = (parents[..., :, None] == indices).astype(jnp.int32)
    identity_map = jnp.broadcast_to((indices[:, None] == indices[None, :]).astype(jnp.int32), step_map.shape)
    reached = identity_map
    hop_map = identity_map
    for step_index in range(prop_count - 1):
        hop_map = jnp.einsum('sij,sjk->sik', hop_map, step_map)
        reached = reached + hop_map
    return reached

def angles(positions):
    halfway = ROPE // 2
    inverse = rope_base ** (-jnp.arange(halfway, dtype=jnp.float32) / halfway)
    angle = positions.astype(jnp.float32)[..., None] * inverse
    return (jnp.cos(angle), jnp.sin(angle))

def rotate(vectors, cosine, sine_part):
    halfway = vectors.shape[-1] // 2
    leading = vectors[..., :halfway]
    trailing = vectors[..., halfway:]
    return jnp.concatenate([leading * cosine - trailing * sine_part, trailing * cosine + leading * sine_part], -1)

def keys_of(latents, rope_rows, w_key_up, key_gain):
    row_count = latents.shape[0]
    nope = jnp.dot(latents, w_key_up, preferred_element_type=jnp.float32).reshape(row_count, HEADS, NOPE)
    rope_wide = jnp.broadcast_to(rope_rows.astype(jnp.float32)[:, None, :], (row_count, HEADS, ROPE))
    joined = jnp.concatenate([nope, rope_wide], -1)
    factor = lax.rsqrt(lax.optimization_barrier(jnp.mean(joined * joined, -1, keepdims=True)) + epsilon)
    return (joined * factor * key_gain).astype(jnp.bfloat16)

def reference(tokens, parents, lengths, accepted, in_gain, w_query, w_latent, w_rope_key, latent_gain, query_gain, key_gain, w_key_up, w_value_up, w_out, out_gain, cache_latent, cache_rope):
    row_count = SEQS * PROPS
    flattened = tokens.reshape(row_count, D).astype(jnp.float32)
    normed = (flattened * lax.rsqrt(lax.optimization_barrier(jnp.mean(flattened * flattened, -1, keepdims=True)) + epsilon) * in_gain).astype(jnp.bfloat16)
    query_raw = jnp.dot(normed, w_query, preferred_element_type=jnp.float32).reshape(SEQS, PROPS, HEADS, QK)
    latent_raw = jnp.dot(normed, w_latent, preferred_element_type=jnp.float32).reshape(SEQS, PROPS, LATENT)
    rope_raw = jnp.dot(normed, w_rope_key, preferred_element_type=jnp.float32).reshape(SEQS, PROPS, ROPE)
    reached = ancestry(parents)
    anchor = (lengths + accepted).astype(jnp.int32)
    positions = anchor[:, None] + lax.optimization_barrier(jnp.sum(reached, -1)) - 1
    cosine, sine_part = angles(positions)
    turned = rotate(query_raw[..., NOPE:], cosine[:, :, None, :], sine_part[:, :, None, :])
    joined = jnp.concatenate([query_raw[..., :NOPE], turned], -1)
    query = (joined * lax.rsqrt(lax.optimization_barrier(jnp.mean(joined * joined, -1, keepdims=True)) + epsilon) * query_gain).astype(jnp.bfloat16)
    latent_new = (latent_raw * lax.rsqrt(lax.optimization_barrier(jnp.mean(latent_raw * latent_raw, -1, keepdims=True)) + epsilon) * latent_gain).astype(jnp.bfloat16)
    rope_new = rotate(rope_raw, cosine, sine_part).astype(jnp.bfloat16)

    def place(table, fresh, start):
        return lax.dynamic_update_slice(table, fresh, (start.astype(jnp.int32), jnp.zeros((), jnp.int32)))
    new_latent = jax.vmap(place)(cache_latent, latent_new, anchor)
    new_rope = jax.vmap(place)(cache_rope, rope_new, anchor)
    score_scale = QK ** (-0.5)

    def attend_one(inputs):
        query_s, latent_s, rope_s, reached_s, anchor_s, cache_lat, cache_rot = inputs
        keys_cache = keys_of(cache_lat, cache_rot, w_key_up, key_gain)
        keys_own = keys_of(latent_s, rope_s, w_key_up, key_gain)
        query_f = query_s.astype(jnp.float32)
        scores_cache = jnp.einsum('phd,lhd->hpl', query_f, keys_cache.astype(jnp.float32)) * score_scale
        visible = jnp.arange(cache_lat.shape[0], dtype=jnp.int32) < anchor_s
        scores_cache = jnp.where(visible[None, None, :], scores_cache, -jnp.inf)
        scores_own = jnp.einsum('phd,khd->hpk', query_f, keys_own.astype(jnp.float32)) * score_scale
        scores_own = jnp.where(reached_s[None] > 0, scores_own, -jnp.inf)
        highest = jnp.maximum(lax.optimization_barrier(jnp.max(scores_cache, -1)), lax.optimization_barrier(jnp.max(scores_own, -1)))
        weights_cache = jnp.exp(scores_cache - highest[..., None])
        weights_own = jnp.exp(scores_own - highest[..., None])
        totals = lax.optimization_barrier(jnp.sum(weights_cache, -1)) + lax.optimization_barrier(jnp.sum(weights_own, -1))
        summed = jnp.einsum('hpl,lc->phc', weights_cache.astype(jnp.bfloat16).astype(jnp.float32), cache_lat.astype(jnp.float32))
        summed = summed + jnp.einsum('hpk,kc->phc', weights_own.astype(jnp.bfloat16).astype(jnp.float32), latent_s.astype(jnp.float32))
        return summed / jnp.transpose(totals)[..., None]
    attended = lax.map(attend_one, (query, latent_new, rope_new, reached, anchor, cache_latent, cache_rope))
    value_up = w_value_up.astype(jnp.float32).reshape(LATENT, HEADS, VDIM)
    values = jnp.einsum('sphc,chd->sphd', attended, value_up, precision=lax.Precision.HIGHEST)
    values_low = values.astype(jnp.bfloat16).reshape(row_count, HEADS * VDIM)
    projected = jnp.dot(values_low, w_out, preferred_element_type=jnp.float32)
    mixed = (projected * lax.rsqrt(lax.optimization_barrier(jnp.mean(projected * projected, -1, keepdims=True)) + epsilon) * out_gain).astype(jnp.bfloat16)
    return (mixed.reshape(SEQS, PROPS, D), new_latent, new_rope)
```

```python
import functools

import jax
import jax.numpy as jnp
import numpy as np
from jax import lax
from jax.experimental import pallas as pl
from jax.experimental.pallas import tpu as pltpu
from jax.sharding import Mesh
from jax.sharding import PartitionSpec as P

D = 4096
NOPE = 64
ROPE = 32
QK = 96
SEQS = 4
PROPS = 4
HEADS = 4
LANES = 128
EPS = 1e-06
KV = ("z", "y")
PLANE = ("y", "x", "c")
F32 = jnp.float32
BF16 = jnp.bfloat16
HIDDEN = -1e30

VMEM = pl.BlockSpec(memory_space=pltpu.VMEM)
SMEM = pl.BlockSpec(memory_space=pltpu.SMEM)


def kernel(body, outs, *args, name, specs=None, flops=2_000_000, traffic=1_000_000):
    shapes = [jax.ShapeDtypeStruct(shape, kind) for shape, kind in outs]
    single = len(shapes) == 1
    return pl.pallas_call(
        body,
        out_shape=shapes[0] if single else shapes,
        in_specs=list(specs) if specs else [VMEM] * len(args),
        out_specs=VMEM if single else [VMEM] * len(shapes),
        cost_estimate=pl.CostEstimate(flops=flops, bytes_accessed=traffic, transcendentals=0),
        name=name,
    )(*args)


def lanes_of(shape):
    return lax.broadcasted_iota(jnp.int32, shape, len(shape) - 1)


def rows_of(shape):
    return lax.broadcasted_iota(jnp.int32, shape, len(shape) - 2)


def matmul(left, right):
    return lax.dot_general(left, right, (((1,), (0,)), ((), ())), preferred_element_type=F32)


def matmul_t(left, right):
    return lax.dot_general(left, right, (((1,), (1,)), ((), ())), preferred_element_type=F32)


def half_pick(low, high):
    shape = jnp.broadcast_shapes(low.shape, high.shape)
    shape = (*shape[:-1], LANES)
    return jnp.where(lanes_of(shape) < NOPE, low, high)


def quarter_pick(parts):
    shape = (*parts[0].shape[:-1], LANES)
    lane = lanes_of(shape)
    return jnp.where(
        lane < NOPE,
        jnp.where(lane < ROPE, parts[0], parts[1]),
        jnp.where(lane < NOPE + ROPE, parts[2], parts[3]),
    )


def head_scales(first, second, rope_squares):
    lane = lanes_of(first.shape)
    found = []
    for h, part in enumerate((first, first, second, second)):
        inside = lane < NOPE if h % 2 == 0 else lane >= NOPE
        squares = jnp.sum(jnp.where(inside, part * part, 0.0), -1, keepdims=True)
        found.append(lax.rsqrt((squares + rope_squares[h]) / QK + EPS))
    return found


def gains(gain_row):
    nope = gain_row[:, :NOPE]
    rope = gain_row[:, NOPE:QK]
    return jnp.concatenate([nope, nope], 1), jnp.concatenate([rope] * 4, 1)


def keys_of(nope, rope_tiled, key_gain):
    first, second = nope[:, :LANES], nope[:, LANES:]
    lane = lanes_of(rope_tiled.shape)
    rope_sum = jnp.sum(jnp.where(lane < ROPE, rope_tiled * rope_tiled, 0.0), -1, keepdims=True)
    scales = head_scales(first, second, [rope_sum] * 4)
    nope_gain, rope_gain = gains(key_gain)
    return (
        first * half_pick(scales[0], scales[1]) * nope_gain,
        second * half_pick(scales[2], scales[3]) * nope_gain,
        rope_tiled * quarter_pick(scales) * rope_gain,
    )


def attend(query, keys, values, seen):
    scale = QK ** (-0.5)
    scores = [jnp.where(v, matmul_t(query, k) * scale, HIDDEN) for k, v in zip(keys, seen)]
    peak = functools.reduce(jnp.maximum, [jnp.max(s, -1, keepdims=True) for s in scores])
    weights = [jnp.where(v, jnp.exp(s - peak), 0.0) for s, v in zip(scores, seen)]
    total = sum(jnp.sum(w, -1, keepdims=True) for w in weights)
    summed = 0.0
    for weight, value in zip(weights, values):
        low = weight.astype(BF16)
        high_part = value.astype(BF16)
        rest = (value - high_part.astype(F32)).astype(BF16)
        summed = summed + matmul(low, high_part) + matmul(low, rest)
    first = half_pick(summed[0:4, :LANES], summed[4:8, :LANES])
    second = half_pick(summed[8:12, LANES:], summed[12:16, LANES:])
    lane = lanes_of((PROPS, LANES))
    peaks = jnp.zeros((PROPS, LANES), F32)
    totals = jnp.zeros((PROPS, LANES), F32)
    for h in range(HEADS):
        peaks = jnp.where(lane == h, peak[4 * h : 4 * h + 4], peaks)
        totals = jnp.where(lane == h, total[4 * h : 4 * h + 4], totals)
    return jnp.concatenate([first, second, peaks, totals], 0)


def sine_cosine(angle):
    turns = jnp.floor(angle * (2.0 / np.pi) + 0.5)
    rest = ((angle - turns * 1.5703125) - turns * 4.837512969970703125e-4) - turns * 7.549789954891882e-8
    square = rest * rest
    sine = rest + rest * square * (
        -1.6666654611e-1 + square * (8.3321608736e-3 + square * -1.9515295891e-4)
    )
    cosine = (
        1.0
        - 0.5 * square
        + square
        * square
        * (4.166664568298827e-2 + square * (-1.388731625493765e-3 + square * 2.443315711809948e-5))
    )
    quadrant = turns - 4.0 * jnp.floor(turns * 0.25)
    odd = (quadrant == 1.0) | (quadrant == 3.0)
    sine_out = jnp.where(odd, cosine, sine)
    cosine_out = jnp.where(odd, sine, cosine)
    sine_out = jnp.where(quadrant >= 2.0, -sine_out, sine_out)
    cosine_out = jnp.where((quadrant == 1.0) | (quadrant == 2.0), -cosine_out, cosine_out)
    return sine_out, cosine_out


def turn(rope_tiled, cosine, sine_a, sine_b):
    return (
        rope_tiled * cosine
        + pltpu.roll(rope_tiled, LANES - 16, 1) * sine_a
        + pltpu.roll(rope_tiled, 16, 1) * sine_b
    )


def ancestors(parents_ref, s):
    masks = []
    for i in range(PROPS):
        mask = jnp.int32(1 << i)
        if i:
            parent = parents_ref[s, i]
            for j in range(i):
                mask = mask + jnp.where(parent == j, masks[j], 0)
        masks.append(mask)
    return masks


def bits(mask):
    return sum((mask >> j) & 1 for j in range(PROPS))


def project_body(tok_ref, gain_ref, wq_ref, wl_ref, out_ref):
    kv = lax.axis_index("z") * lax.axis_size("y") + lax.axis_index("y")
    rows = wq_ref.shape[0]
    width = max(rows, LANES)
    per = width // rows
    base = pl.multiple_of((kv // per) * width, LANES)
    parts = []
    for s in range(SEQS):
        tok = tok_ref[s].astype(F32)
        scale = lax.rsqrt(jnp.sum(tok * tok, -1, keepdims=True) / D + EPS)
        piece = tok_ref[s, :, pl.ds(base, width)].astype(F32)
        parts.append(piece * scale * gain_ref[:, pl.ds(base, width)])
    part = jnp.concatenate(parts, 0)
    if per > 1:
        part = jnp.where(lanes_of(part.shape) // rows == kv % per, part, 0.0)
    part = part.astype(BF16)
    wq = jnp.concatenate([wq_ref[...]] * per, 0)
    half = wl_ref.shape[1] // 2
    wl = wl_ref[:, pl.ds(pl.multiple_of(lax.axis_index("c") * half, LANES), half)]
    wl = jnp.concatenate([wl] * per, 0)
    query = matmul(part, wq)
    latent = matmul(part, wl)
    nope = [query[:, QK * h : QK * h + NOPE] for h in range(HEADS)]
    rope = [query[:, QK * h + NOPE : QK * h + QK] for h in range(HEADS)]
    chunks = [
        jnp.concatenate(nope[:2], 1),
        jnp.concatenate(nope[2:], 1),
        jnp.concatenate(rope, 1),
    ] + [latent[:, LANES * k : LANES * k + LANES] for k in range(half // LANES)]
    for s in range(SEQS):
        for k, chunk in enumerate(chunks):
            out_ref[s, 4 * k : 4 * k + 4, :] = chunk[4 * s : 4 * s + 4]
        out_ref[s, 28:32, :] = jnp.zeros((4, LANES), F32)


def relay_body(in_ref, out_ref):
    total = in_ref[0]
    for k in range(1, in_ref.shape[0]):
        total = total + in_ref[k]
    for k in range(out_ref.shape[0]):
        out_ref[k] = total


def angles_body(
    parents_ref, lengths_ref, accepted_ref, tok_ref, gain_ref, wr_ref, inverse_ref, rope_ref, flipped_ref, cos_ref, a_ref, b_ref
):
    row = rows_of((16, LANES))
    position = jnp.zeros((16, LANES), F32)
    parts = []
    for s in range(SEQS):
        anchor = lengths_ref[s] + accepted_ref[s]
        for i, mask in enumerate(ancestors(parents_ref, s)):
            place = (anchor + bits(mask) - 1).astype(F32)
            position = jnp.where(row == 4 * s + i, place, position)
        tok = tok_ref[s].astype(F32)
        scale = lax.rsqrt(jnp.sum(tok * tok, -1, keepdims=True) / D + EPS)
        parts.append(tok * scale * gain_ref[...])
    normed = jnp.concatenate(parts, 0).astype(BF16)
    raw = matmul_t(normed, wr_ref[...])
    raw = jnp.concatenate([raw] * 4, 1)
    sine, cosine = sine_cosine(position * inverse_ref[...])
    early = lanes_of((16, LANES)) % ROPE < 16
    sine_a = jnp.where(early, -sine, 0.0)
    sine_b = jnp.where(early, 0.0, sine)
    rope = turn(raw, cosine, sine_a, sine_b)
    for s in range(SEQS):
        rope_ref[s] = rope[4 * s : 4 * s + 4]
        cos_ref[s] = cosine[4 * s : 4 * s + 4]
        a_ref[s] = sine_a[4 * s : 4 * s + 4]
        b_ref[s] = sine_b[4 * s : 4 * s + 4]
    tall = jnp.concatenate([rope, jnp.zeros((LANES - 16, LANES), F32)], 0)
    flipped_ref[...] = tall.T[:ROPE]


def blocks_body(latent_ref, rope_ref, wk_ref, wv_ref, gain_ref, wo_ref, *out_refs):
    y = lax.axis_index("y")
    weights = wo_ref[...].astype(F32)
    for k, out_ref in enumerate(out_refs):
        s = lax.rem(y + k, SEQS)
        latent = latent_ref[s]
        nope = matmul(latent, wk_ref[...])
        rope = rope_ref[s].astype(F32)
        tiled = jnp.concatenate([rope] * 4, 0).T
        for j, part in enumerate(keys_of(nope, tiled, gain_ref[...])):
            out_ref[:, LANES * j : LANES * j + LANES] = part
        out_ref[:, 384:640] = matmul(latent, wv_ref[...])
        out_ref[0:64, 640:768] = weights[:, :LANES]
        out_ref[64:128, 640:768] = weights[:, LANES:]


def query_body(in_ref, cos_ref, a_ref, b_ref, gain_ref, query_ref, latent_ref):
    y = lax.axis_index("y")
    total = in_ref[0]
    for k in range(1, in_ref.shape[0]):
        total = total + in_ref[k]
    first, second = total[0:4], total[4:8]
    rope = turn(total[8:12], cos_ref[y], a_ref[y], b_ref[y])
    lane = lanes_of(rope.shape)
    sums = [
        jnp.sum(jnp.where(lane // ROPE == h, rope * rope, 0.0), -1, keepdims=True)
        for h in range(HEADS)
    ]
    scales = head_scales(first, second, sums)
    nope_gain, rope_gain = gains(gain_ref[...])
    first = first * half_pick(scales[0], scales[1]) * nope_gain
    second = second * half_pick(scales[2], scales[3]) * nope_gain
    rope = rope * quarter_pick(scales) * rope_gain
    for h in range(HEADS):
        inside = (lane < NOPE) if h % 2 == 0 else (lane >= NOPE)
        empty = jnp.zeros_like(first)
        query_ref[4 * h : 4 * h + 4, 0:128] = jnp.where(inside, first, 0.0) if h < 2 else empty
        query_ref[4 * h : 4 * h + 4, 128:256] = jnp.where(inside, second, 0.0) if h >= 2 else empty
        query_ref[4 * h : 4 * h + 4, 256:384] = jnp.where(lane // ROPE == h, rope, 0.0)
    latent_ref[...] = total[12:28]


def own_body(parents_ref, latent_ref, gain_ref, rope_ref, query_ref, wk_ref, wv_ref, kgain_ref, fresh_ref, out_ref):
    y = lax.axis_index("y")
    pieces = [latent_ref[c, 4 * k : 4 * k + 4] for c in range(2) for k in range(4)]
    raw = jnp.concatenate(pieces, 1)
    scale = lax.rsqrt(jnp.sum(raw * raw, -1, keepdims=True) / raw.shape[1] + EPS)
    fresh = raw * scale * gain_ref[...]
    fresh_ref[...] = fresh
    low = jnp.concatenate([fresh, jnp.zeros_like(fresh)], 0).astype(BF16)
    nope = matmul(low, wk_ref[...])
    value = matmul(low, wv_ref[...])
    rope = rope_ref[y].astype(BF16).astype(F32)
    tiled = jnp.concatenate([rope, jnp.zeros_like(rope)], 0)
    key = jnp.concatenate(keys_of(nope, tiled, kgain_ref[...]), 1)
    key = jnp.concatenate([key, jnp.zeros((LANES - 8, 384), F32)], 0).astype(BF16)
    value = jnp.concatenate([value, jnp.zeros((LANES - 8, 256), F32)], 0)
    masks = ancestors(parents_ref, y)
    shape = (16, LANES)
    prop, lane = rows_of(shape) % PROPS, lanes_of(shape)
    seen = jnp.zeros(shape, jnp.int32)
    for i in range(PROPS):
        for j in range(i + 1):
            seen = jnp.where((prop == i) & (lane == j), (masks[i] >> j) & 1, seen)
    out_ref[...] = attend(query_ref[...].astype(BF16), [key], [value], [seen > 0])


def attend_body(lengths_ref, accepted_ref, query_ref, *refs):
    block_refs, out_ref = refs[:-1], refs[-1]
    y = lax.axis_index("y")
    size = SEQS
    anchor = lengths_ref[y] + accepted_ref[y]
    keys, values, seen = [], [], []
    for k, block_ref in enumerate(block_refs):
        rows = block_ref.shape[0]
        start = (lax.axis_index("z") * size + lax.rem(y + size - k, size)) * rows
        keys.append(block_ref[:, 0:384].astype(BF16))
        values.append(block_ref[:, 384:640])
        seen.append(lanes_of((16, rows)) + start < anchor)
    packed = attend(query_ref[...].astype(BF16), keys, values, seen)
    for k in range(out_ref.shape[0]):
        out_ref[k] = packed


def merge_body(in_ref, own_ref, fresh_ref, *refs):
    weight_refs, out_ref = refs[:-1], refs[-1]
    y = lax.axis_index("y")
    share = lax.axis_index("x") * lax.axis_size("c") + lax.axis_index("c")
    parts = [in_ref[k] for k in range(in_ref.shape[0])] + [own_ref[...]]
    peak = functools.reduce(jnp.maximum, [p[8:12] for p in parts])
    first = second = total = 0.0
    for p in parts:
        scale = jnp.exp(p[8:12] - peak)
        total = total + p[12:16] * scale
        first = first + p[0:4] * half_pick(scale[:, 0:1], scale[:, 1:2])
        second = second + p[4:8] * half_pick(scale[:, 2:3], scale[:, 3:4])
    first = first / half_pick(total[:, 0:1], total[:, 1:2])
    second = second / half_pick(total[:, 2:3], total[:, 3:4])
    pad = jnp.zeros((4, LANES), F32)
    first = jnp.concatenate([first, pad], 0).astype(BF16)
    second = jnp.concatenate([second, pad], 0).astype(BF16)
    sums = [jnp.zeros((8, LANES), F32) for _ in range(4)]
    for k, weight_ref in enumerate(weight_refs):
        weight = weight_ref[...].astype(BF16)
        low = matmul_t(first, weight) + pltpu.roll(matmul_t(second, weight), NOPE, 1)
        both = half_pick(low, pltpu.roll(low, NOPE, 1))
        place = lax.rem(y + SEQS - k, SEQS)
        sums = [jnp.where(place == j, both, sums[j]) for j in range(4)]
    latent = fresh_ref[:, pl.ds(pl.multiple_of(share * LANES, LANES), LANES)]
    packed = jnp.concatenate(
        [half_pick(sums[0], sums[1])[0:4], half_pick(sums[2], sums[3])[0:4], latent, pad], 0
    )
    for k in range(out_ref.shape[0]):
        out_ref[k] = packed


def gather_body(in_ref, own_ref, square_ref, latent_ref):
    y = lax.axis_index("y")
    peers = in_ref.shape[0] // SEQS
    lane = lanes_of((PROPS, LANES))
    squares = jnp.zeros((PROPS, LANES), F32)
    for s in range(SEQS):
        total = in_ref[peers * s, 0:8]
        for t in range(1, peers):
            total = total + in_ref[peers * s + t, 0:8]
        first, second = total[0:4], total[4:8]
        square = jnp.sum(first * first + second * second, -1, keepdims=True)
        squares = jnp.where(lane == s, square, squares)
        picked = jnp.where(y < 2, first, second)
        own_ref[s] = jnp.where(lax.rem(y, 2) == 0, picked, pltpu.roll(picked, NOPE, 1))
        for t in range(peers):
            latent_ref[s, :, LANES * t : LANES * t + LANES] = in_ref[peers * s + t, 8:12]
    packed = jnp.concatenate([squares, jnp.zeros_like(squares)], 0)
    for k in range(square_ref.shape[0]):
        square_ref[k] = packed


def finish_body(in_ref, own_ref, gain_ref, out_ref):
    total = in_ref[0]
    for k in range(1, in_ref.shape[0]):
        total = total + in_ref[k]
    for s in range(SEQS):
        scale = lax.rsqrt(total[0:4, s : s + 1] / D + EPS)
        out_ref[s] = (own_ref[s, :, :NOPE] * scale * gain_ref[...]).astype(BF16)


def write_body(lengths_ref, accepted_ref, cache_ref, rope_ref, fresh_ref, flipped_ref, out_ref, rope_out_ref):
    kv = lax.axis_index("z") * lax.axis_size("y") + lax.axis_index("y")
    rows = cache_ref.shape[1]
    out_ref[...] = cache_ref[...]
    for s in range(SEQS):
        start = lengths_ref[s] + accepted_ref[s] - kv * rows
        rope = rope_ref[s].astype(F32)
        lane = lanes_of(rope.shape)
        for p in range(PROPS):
            rope = jnp.where(lane == start + p, flipped_ref[:, 4 * s + p : 4 * s + p + 1], rope)
        rope_out_ref[s] = rope.astype(BF16)

        @pl.when((start > -PROPS) & (start < rows))
        def _(s=s, start=start):
            base = jnp.clip(start // 16, 0, rows // 16 - 2) * 16
            base = pl.multiple_of(base, 16)
            window = out_ref[s, pl.ds(base, 32), :].astype(F32)
            row = rows_of(window.shape) + base
            for p in range(PROPS):
                window = jnp.where(row == start + p, fresh_ref[s, p : p + 1, :], window)
            out_ref[s, pl.ds(base, 32), :] = window.astype(BF16)


def swap(parts, axis):
    return lax.all_to_all(parts, axis, split_axis=0, concat_axis=0, tiled=True)


def body(
    tokens,
    parents,
    lengths,
    accepted,
    in_gain,
    w_query,
    w_latent,
    w_rope_key,
    latent_gain,
    query_gain,
    key_gain,
    w_key_up,
    w_value_up,
    w_out,
    out_gain,
    cache_latent,
    cache_rope,
):
    depth, tall = lax.axis_size("z"), lax.axis_size("y")
    plane = lax.axis_size(PLANE)
    in_row, latent_row = in_gain.reshape(1, -1), latent_gain.reshape(1, -1)
    query_row, key_row = query_gain.reshape(1, -1), key_gain.reshape(1, -1)
    inverse = 10000.0 ** (-(np.arange(LANES) % 16).astype(np.float32) / 16)
    inverse = jnp.asarray(inverse.astype(np.float32).reshape(1, LANES))
    rope_cols = jnp.swapaxes(cache_rope, 1, 2)
    positions = cache_latent.shape[1]

    sent = kernel(
        project_body, [((tall, 32, LANES), F32)], tokens, in_row, w_query, w_latent, name="project"
    )
    reduced = swap(sent, "y")
    spread = kernel(relay_body, [((depth, 32, LANES), F32)], reduced, name="relay")
    gathered = swap(spread, "z")

    blocks = kernel(
        blocks_body,
        [((positions, 768), F32)] * SEQS,
        cache_latent,
        rope_cols,
        w_key_up,
        w_value_up,
        key_row,
        w_out.T,
        name="blocks",
        flops=540_000_000,
        traffic=5_000_000,
    )
    arrived = [blocks[0]]
    for k in range(1, SEQS):
        pairs = [(i, (i + k) % SEQS) for i in range(SEQS)]
        arrived.append(lax.ppermute(blocks[k], "y", pairs))
    rope_new, rope_flipped, cosine, sine_a, sine_b = kernel(
        angles_body,
        [((SEQS, PROPS, LANES), F32), ((ROPE, LANES), F32)] + [((SEQS, PROPS, LANES), F32)] * 3,
        parents,
        lengths,
        accepted,
        tokens,
        in_row,
        w_rope_key.T,
        inverse,
        name="angles",
        specs=[SMEM] * 3 + [VMEM] * 4,
    )

    query, latent_half = kernel(
        query_body,
        [((16, 384), F32), ((16, LANES), F32)],
        gathered,
        cosine,
        sine_a,
        sine_b,
        query_row,
        name="query",
    )
    latent_both = lax.all_gather(latent_half, "c")
    fresh, own = kernel(
        own_body,
        [((PROPS, 1024), F32), ((16, LANES), F32)],
        parents,
        latent_both,
        latent_row,
        rope_new,
        query,
        w_key_up,
        w_value_up,
        key_row,
        name="own",
        specs=[SMEM] + [VMEM] * 7,
    )
    partial = kernel(
        attend_body,
        [((depth, 16, LANES), F32)],
        lengths,
        accepted,
        query,
        *arrived,
        name="attend",
        specs=[SMEM] * 2 + [VMEM] * 5,
    )
    partials = swap(partial, "z")
    projected = kernel(
        merge_body,
        [((plane, 16, LANES), F32)],
        partials,
        own,
        fresh,
        *[a[:, 640:768] for a in arrived],
        name="merge",
    )
    projections = swap(projected, PLANE)
    own_columns, squares, fresh_all = kernel(
        gather_body,
        [((SEQS, PROPS, LANES), F32), ((depth, 8, LANES), F32), ((SEQS, PROPS, 1024), F32)],
        projections,
        name="gather",
    )
    square_parts = swap(squares, "z")
    new_latent, new_rope = kernel(
        write_body,
        [(cache_latent.shape, BF16), (rope_cols.shape, BF16)],
        lengths,
        accepted,
        cache_latent,
        rope_cols,
        fresh_all,
        rope_flipped,
        name="write",
        specs=[SMEM] * 2 + [VMEM] * 4,
    )
    mixed = kernel(
        finish_body,
        [((SEQS, PROPS, NOPE), BF16)],
        square_parts,
        own_columns,
        out_gain.reshape(1, -1),
        name="finish",
    )
    return (mixed, new_latent, jnp.swapaxes(new_rope, 1, 2))


def solution(mesh):
    kv, tp = mesh.shape["kv"], mesh.shape["tp"]
    finer = Mesh(mesh.devices.reshape(kv // 4, 4, tp // 2, 2), ("z", "y", "x", "c"))
    tp_axes = ("x", "c")
    placed = (
        P(),
        P(),
        P(),
        P(),
        P(),
        P(KV, tp_axes),
        P(KV, None),
        P(),
        P(),
        P(),
        P(),
        P(None, tp_axes),
        P(None, tp_axes),
        P(tp_axes, KV),
        P(KV),
        P(None, KV, None),
        P(None, KV, None),
    )
    return jax.shard_map(
        body,
        mesh=finer,
        in_specs=placed,
        out_specs=(P(None, None, KV), P(None, KV, None), P(None, KV, None)),
        check_vma=False,
    )
```

```python
import functools

import jax
import jax.numpy as jnp
import numpy as np
from jax import lax
from jax.experimental import pallas as pl
from jax.experimental.pallas import tpu as pltpu
from jax.sharding import Mesh
from jax.sharding import PartitionSpec as P


D = 4096
NOPE = 64
ROPE = 32
QK = 96
SEQS = 4
PROPS = 4
HEADS = 4
LANES = 128
EPS = 1e-06
KV = ("z", "y")
PLANE = ("y", "x", "c")
F32 = jnp.float32
BF16 = jnp.bfloat16
HIDDEN = -1e30

VMEM = pl.BlockSpec(memory_space=pltpu.VMEM)
HBM = pl.BlockSpec(memory_space=pltpu.HBM)
CHUNKS = 7
TURN_AT, SCALE_AT, VALUE_AT, WEIGHT_AT, BLOCK_ROWS = 256, 288, 296, 552, 680
ROPE_AT, COS_AT, A_AT, B_AT, SEEN_AT, ANCHOR_AT = 0, 4, 8, 12, 16, 32
QN_AT, QR_AT, KN_AT, KR_AT, OUT_AT, START_AT, LATENT_AT = 33, 34, 35, 36, 37, 38, 40
GAIN_AT, TABLE_ROWS = 48, 144
WINDOW = 32


def kernel(body, outs, *args, specs=None, out_specs=None, scratch=(), aliases=None, mebibytes=8):
    shapes = [jax.ShapeDtypeStruct(shape, kind) for shape, kind in outs]
    out_specs = list(out_specs) if out_specs else [VMEM] * len(shapes)
    single = len(shapes) == 1
    return pl.pallas_call(
        body,
        out_shape=shapes[0] if single else shapes,
        in_specs=list(specs) if specs else [VMEM] * len(args),
        out_specs=out_specs[0] if single else out_specs,
        scratch_shapes=list(scratch),
        input_output_aliases=aliases or {},
        cost_estimate=pl.CostEstimate(flops=2_000_000, bytes_accessed=1_000_000, transcendentals=0),
        compiler_params=pltpu.CompilerParams(vmem_limit_bytes=mebibytes * 2**20),
    )(*args)


def lanes_of(shape):
    return lax.broadcasted_iota(jnp.int32, shape, len(shape) - 1)


def rows_of(shape):
    return lax.broadcasted_iota(jnp.int32, shape, len(shape) - 2)


def matmul(left, right):
    return lax.dot_general(left, right, (((1,), (0,)), ((), ())), preferred_element_type=F32)


def matmul_t(left, right):
    return lax.dot_general(left, right, (((1,), (1,)), ((), ())), preferred_element_type=F32)


def half_pick(low, high):
    shape = jnp.broadcast_shapes(low.shape, high.shape)
    shape = (*shape[:-1], LANES)
    return jnp.where(lanes_of(shape) < NOPE, low, high)


def quarter_pick(parts):
    shape = (*parts[0].shape[:-1], LANES)
    lane = lanes_of(shape)
    return jnp.where(
        lane < NOPE,
        jnp.where(lane < ROPE, parts[0], parts[1]),
        jnp.where(lane < NOPE + ROPE, parts[2], parts[3]),
    )


def head_scales(first, second, rope_squares):
    lane = lanes_of(first.shape)
    found = []
    for h, part in enumerate((first, first, second, second)):
        inside = lane < NOPE if h % 2 == 0 else lane >= NOPE
        squares = jnp.sum(jnp.where(inside, part * part, 0.0), -1, keepdims=True)
        found.append(lax.rsqrt((squares + rope_squares[h]) / QK + EPS))
    return found


def gains(gain_row):
    nope = gain_row[:, :NOPE]
    rope = gain_row[:, NOPE:QK]
    return jnp.concatenate([nope, nope], 1), jnp.concatenate([rope] * 4, 1)


def keys_of(nope, rope_tiled, nope_gain, rope_gain):
    first, second = nope[:, :LANES], nope[:, LANES:]
    lane = lanes_of(rope_tiled.shape)
    rope_sum = jnp.sum(jnp.where(lane < ROPE, rope_tiled * rope_tiled, 0.0), -1, keepdims=True)
    scales = head_scales(first, second, [rope_sum] * 4)
    return (
        first * half_pick(scales[0], scales[1]) * nope_gain,
        second * half_pick(scales[2], scales[3]) * nope_gain,
        rope_tiled * quarter_pick(scales) * rope_gain,
    )


def attend(products, values, seen):
    scale = QK ** (-0.5)
    scores = [jnp.where(v, p * scale, HIDDEN) for p, v in zip(products, seen)]
    peak = functools.reduce(jnp.maximum, [jnp.max(s, -1, keepdims=True) for s in scores])
    weights = [jnp.where(v, jnp.exp(s - peak), 0.0) for s, v in zip(scores, seen)]
    total = sum(jnp.sum(w, -1, keepdims=True) for w in weights)
    sums = [0.0, 0.0]
    for weight, value in zip(weights, values):
        low = weight.astype(BF16)
        for j, part in enumerate(value):
            high_part = part.astype(BF16)
            rest = (part - high_part.astype(F32)).astype(BF16)
            sums[j] = sums[j] + matmul(low, high_part) + matmul(low, rest)
    first = half_pick(sums[0][0:4], sums[0][4:8])
    second = half_pick(sums[1][8:12], sums[1][12:16])
    lane = lanes_of((PROPS, LANES))
    stats = jnp.zeros((PROPS, LANES), F32)
    for h in range(HEADS):
        stats = jnp.where(lane == h, peak[4 * h : 4 * h + 4], stats)
        stats = jnp.where(lane == HEADS + h, total[4 * h : 4 * h + 4], stats)
    return first, second, stats


def sine_cosine(angle):
    turns = jnp.floor(angle * (2.0 / np.pi) + 0.5)
    rest = ((angle - turns * 1.5703125) - turns * 4.837512969970703125e-4) - turns * 7.549789954891882e-8
    square = rest * rest
    sine = rest + rest * square * (
        -1.6666654611e-1 + square * (8.3321608736e-3 + square * -1.9515295891e-4)
    )
    cosine = (
        1.0
        - 0.5 * square
        + square
        * square
        * (4.166664568298827e-2 + square * (-1.388731625493765e-3 + square * 2.443315711809948e-5))
    )
    quadrant = turns - 4.0 * jnp.floor(turns * 0.25)
    odd = (quadrant == 1.0) | (quadrant == 3.0)
    sine_out = jnp.where(odd, cosine, sine)
    cosine_out = jnp.where(odd, sine, cosine)
    sine_out = jnp.where(quadrant >= 2.0, -sine_out, sine_out)
    cosine_out = jnp.where((quadrant == 1.0) | (quadrant == 2.0), -cosine_out, cosine_out)
    return sine_out, cosine_out


def turn(rope_tiled, cosine, sine_a, sine_b):
    return (
        rope_tiled * cosine
        + pltpu.roll(rope_tiled, LANES - 16, 1) * sine_a
        + pltpu.roll(rope_tiled, 16, 1) * sine_b
    )


def ancestors(parents_ref, s):
    masks = []
    for i in range(PROPS):
        mask = jnp.int32(1 << i)
        if i:
            parent = parents_ref[s, i]
            for j in range(i):
                mask = mask + jnp.where(parent == j, masks[j], 0)
        masks.append(mask)
    return masks


def bits(mask):
    return sum((mask >> j) & 1 for j in range(PROPS))


def start_body(
    parents_hbm,
    lengths_hbm,
    accepted_hbm,
    tok_hbm,
    gain_hbm,
    wq_hbm,
    wl_hbm,
    wr_hbm,
    inverse_hbm,
    lgain_hbm,
    qgain_hbm,
    kgain_hbm,
    ogain_hbm,
    wo_hbm,
    rope_hbm,
    wk_hbm,
    wv_hbm,
    cache_hbm,
    out_ref,
    block_0,
    block_1,
    block_2,
    block_3,
    table_ref,
    window_ref,
    rope_out_ref,
    copy_hbm,
    parents_ref,
    lengths_ref,
    accepted_ref,
    tok_ref,
    gain_ref,
    wq_ref,
    wl_ref,
    wr_ref,
    inverse_ref,
    lgain_ref,
    qgain_ref,
    kgain_ref,
    ogain_ref,
    wo_ref,
    rope_ref,
    wk_ref,
    wv_ref,
    cache_ref,
    sems,
):
    sources = (
        parents_hbm, lengths_hbm, accepted_hbm, tok_hbm, gain_hbm, wq_hbm, wl_hbm, wr_hbm, inverse_hbm,
        lgain_hbm, qgain_hbm, kgain_hbm, ogain_hbm, wo_hbm, rope_hbm, wk_hbm, wv_hbm, cache_hbm,
    )
    targets = (
        parents_ref, lengths_ref, accepted_ref, tok_ref, gain_ref, wq_ref, wl_ref, wr_ref, inverse_ref,
        lgain_ref, qgain_ref, kgain_ref, ogain_ref, wo_ref, rope_ref, wk_ref, wv_ref, cache_ref,
    )
    copies = [pltpu.make_async_copy(a, b, sems.at[k]) for k, (a, b) in enumerate(zip(sources, targets))]
    for copy in copies:
        copy.start()
    for copy in copies[:-4]:
        copy.wait()
    y = lax.axis_index("y")
    kv = lax.axis_index("z") * lax.axis_size("y") + y
    rows = wq_ref.shape[0]
    width = max(rows, LANES)
    per = width // rows
    base = pl.multiple_of((kv // per) * width, LANES)
    positions = cache_ref.shape[1]

    parts, normed = [], []
    for s in range(SEQS):
        tok = tok_ref[s].astype(F32)
        scale = lax.rsqrt(jnp.sum(tok * tok, -1, keepdims=True) / D + EPS)
        normed.append(tok * scale * gain_ref[...])
        piece = tok_ref[s, :, pl.ds(base, width)].astype(F32)
        parts.append(piece * scale * gain_ref[:, pl.ds(base, width)])
    part = jnp.concatenate(parts, 0)
    if per > 1:
        part = jnp.where(lanes_of(part.shape) // rows == kv % per, part, 0.0)
    part = part.astype(BF16)
    half = wl_ref.shape[1] // 2
    wl = wl_ref[:, pl.ds(pl.multiple_of(lax.axis_index("c") * half, LANES), half)]
    query = matmul(part, jnp.concatenate([wq_ref[...]] * per, 0))
    latent = matmul(part, jnp.concatenate([wl] * per, 0))
    nope = [query[:, QK * h : QK * h + NOPE] for h in range(HEADS)]
    rope = [query[:, QK * h + NOPE : QK * h + QK] for h in range(HEADS)]
    chunks = [
        jnp.concatenate(nope[:2], 1),
        jnp.concatenate(nope[2:], 1),
        jnp.concatenate(rope, 1),
    ] + [latent[:, LANES * k : LANES * k + LANES] for k in range(half // LANES)]
    for s in range(SEQS):
        for k, chunk in enumerate(chunks):
            out_ref[s, k] = chunk[4 * s : 4 * s + 4]

    row = rows_of((16, LANES))
    place = jnp.zeros((16, LANES), F32)
    starts = []
    for s in range(SEQS):
        anchor = lengths_ref[s] + accepted_ref[s]
        starts.append(anchor - kv * positions)
        for i, mask in enumerate(ancestors(parents_ref, s)):
            place = jnp.where(row == 4 * s + i, (anchor + bits(mask) - 1).astype(F32), place)
    raw = matmul_t(jnp.concatenate(normed, 0).astype(BF16), wr_ref[...])
    raw = jnp.concatenate([raw] * 4, 1)
    sine, cosine = sine_cosine(place * inverse_ref[...])
    early = lanes_of((16, LANES)) % ROPE < 16
    sine_a = jnp.where(early, -sine, 0.0)
    sine_b = jnp.where(early, 0.0, sine)
    fresh = turn(raw, cosine, sine_a, sine_b)
    for at, full in ((ROPE_AT, fresh), (COS_AT, cosine), (A_AT, sine_a), (B_AT, sine_b)):
        own = full[0:4]
        for s in range(1, SEQS):
            own = jnp.where(y == s, full[4 * s : 4 * s + 4], own)
        table_ref[at : at + 4] = own
    masks = ancestors(parents_ref, y)
    prop, lane = row % PROPS, lanes_of((16, LANES))
    seen = jnp.zeros((16, LANES), jnp.int32)
    for i in range(PROPS):
        for j in range(i + 1):
            seen = jnp.where((prop == i) & (lane == j), (masks[i] >> j) & 1, seen)
    table_ref[SEEN_AT : SEEN_AT + 16] = seen.astype(F32)
    anchor = (lengths_ref[y] + accepted_ref[y]).astype(F32)
    table_ref[ANCHOR_AT : ANCHOR_AT + 1] = jnp.zeros((1, LANES), F32) + anchor
    nope_gain, rope_gain = gains(kgain_ref[...])
    table_ref[KN_AT : KN_AT + 1], table_ref[KR_AT : KR_AT + 1] = nope_gain, rope_gain
    table_ref[QN_AT : QN_AT + 1], table_ref[QR_AT : QR_AT + 1] = gains(qgain_ref[...])
    table_ref[OUT_AT : OUT_AT + 1] = jnp.concatenate([ogain_ref[...]] * (LANES // ogain_ref.shape[1]), 1)
    spot = lanes_of((2, LANES))
    begun = jnp.zeros((2, LANES), F32)
    for s in range(SEQS):
        begun = jnp.where(spot == s, starts[s].astype(F32), begun)
    table_ref[START_AT : START_AT + 2] = begun
    for k in range(8):
        table_ref[LATENT_AT + k : LATENT_AT + k + 1] = lgain_ref[:, LANES * k : LANES * k + LANES]
    tall_gain = jnp.concatenate([nope_gain, rope_gain, jnp.zeros((6, LANES), F32)], 0)
    tall_gain = jnp.concatenate([tall_gain] * (LANES // 8), 0).T
    table_ref[GAIN_AT : GAIN_AT + NOPE] = jnp.zeros((NOPE, LANES), F32) + tall_gain[:NOPE, 0:1]
    table_ref[GAIN_AT + NOPE : GAIN_AT + QK] = jnp.zeros((ROPE, LANES), F32) + tall_gain[:ROPE, 1:2]
    flipped = jnp.concatenate([fresh, jnp.zeros((LANES - 16, LANES), F32)], 0).T[:ROPE]

    for copy in copies[-4:]:
        copy.wait()
    kept = pltpu.make_async_copy(cache_ref, copy_hbm, sems.at[len(copies)])
    kept.start()
    weights = wo_ref[...].astype(F32)
    for k, block_ref in enumerate((block_0, block_1, block_2, block_3)):
        s = lax.rem(y + k, SEQS)
        block = cache_ref[s]
        nope = matmul(block, wk_ref[...])
        value = matmul(block, wv_ref[...])
        old = rope_ref[s].astype(F32)
        old_sum = jnp.sum(old * old, 0, keepdims=True)
        block_ref[TURN_AT : TURN_AT + ROPE] = old
        for j in range(2):
            flat = nope[:, LANES * j : LANES * j + LANES].T
            block_ref[LANES * j : LANES * j + LANES] = flat
            block_ref[VALUE_AT + LANES * j : VALUE_AT + LANES * j + LANES] = value[:, LANES * j : LANES * j + LANES]
            for i in range(2):
                dims = flat[NOPE * i : NOPE * i + NOPE]
                squares = jnp.sum(dims * dims, 0, keepdims=True) + old_sum
                h = SCALE_AT + 2 * j + i
                block_ref[h : h + 1] = lax.rsqrt(squares / QK + EPS)
        block_ref[SCALE_AT + 4 : SCALE_AT + 8] = jnp.zeros((4, LANES), F32)
        block_ref[WEIGHT_AT : WEIGHT_AT + 64] = weights[:, :LANES]
        block_ref[WEIGHT_AT + 64 : WEIGHT_AT + 128] = weights[:, LANES:]
    for s in range(SEQS):
        old = rope_ref[s].astype(F32)
        spot = lanes_of(old.shape)
        for p in range(PROPS):
            old = jnp.where(spot == starts[s] + p, flipped[:, 4 * s + p : 4 * s + p + 1], old)
        rope_out_ref[s] = old.astype(BF16)
        window_ref[s] = cache_ref[s, pl.ds(window_base(starts[s], positions), WINDOW), :]
    kept.wait()


def window_base(start, positions):
    return pl.multiple_of(jnp.clip(start // 16, 0, positions // 16 - WINDOW // 16) * 16, 16)


def relay_body(in_ref, out_ref):
    total = in_ref[0]
    for k in range(1, in_ref.shape[0]):
        total = total + in_ref[k]
    for k in range(out_ref.shape[0]):
        out_ref[k] = total


def query_body(in_ref, table_ref, query_ref, latent_ref):
    total = in_ref[0]
    for k in range(1, in_ref.shape[0]):
        total = total + in_ref[k]
    first, second = total[0], total[1]
    rope = turn(
        total[2],
        table_ref[COS_AT : COS_AT + 4],
        table_ref[A_AT : A_AT + 4],
        table_ref[B_AT : B_AT + 4],
    )
    lane = lanes_of(rope.shape)
    sums = [
        jnp.sum(jnp.where(lane // ROPE == h, rope * rope, 0.0), -1, keepdims=True)
        for h in range(HEADS)
    ]
    scales = head_scales(first, second, sums)
    nope_gain, rope_gain = table_ref[QN_AT : QN_AT + 1], table_ref[QR_AT : QR_AT + 1]
    first = first * half_pick(scales[0], scales[1]) * nope_gain
    second = second * half_pick(scales[2], scales[3]) * nope_gain
    rope = rope * quarter_pick(scales) * rope_gain
    for h in range(HEADS):
        inside = (lane < NOPE) if h % 2 == 0 else (lane >= NOPE)
        empty = jnp.zeros_like(first)
        query_ref[0, 4 * h : 4 * h + 4] = jnp.where(inside, first, 0.0) if h < 2 else empty
        query_ref[1, 4 * h : 4 * h + 4] = jnp.where(inside, second, 0.0) if h >= 2 else empty
        query_ref[2, 4 * h : 4 * h + 4] = jnp.where(lane // ROPE == h, rope, 0.0)
    latent_ref[...] = total[3:CHUNKS]


def attend_body(latent_ref, table_ref, query_ref, wk_ref, wv_ref, *refs):
    block_refs, (out_ref, own_ref, fresh_ref) = refs[:SEQS], refs[SEQS:]
    query = [query_ref[j].astype(BF16) for j in range(3)]
    pieces = [latent_ref[c, k] for c in range(2) for k in range(4)]
    squares = sum(jnp.sum(piece * piece, -1, keepdims=True) for piece in pieces)
    scale = lax.rsqrt(squares / (8 * LANES) + EPS)
    pieces = [p * scale * table_ref[LATENT_AT + k : LATENT_AT + k + 1] for k, p in enumerate(pieces)]
    for k, piece in enumerate(pieces):
        fresh_ref[k] = piece
    fresh = jnp.concatenate(pieces, 1)
    low = jnp.concatenate([fresh, jnp.zeros_like(fresh)], 0).astype(BF16)
    value = matmul(low, wv_ref[...])
    rope = table_ref[ROPE_AT : ROPE_AT + 4].astype(BF16).astype(F32)
    tiled = jnp.concatenate([rope, jnp.zeros_like(rope)], 0)
    key = keys_of(
        matmul(low, wk_ref[...]), tiled, table_ref[KN_AT : KN_AT + 1], table_ref[KR_AT : KR_AT + 1]
    )
    pad = jnp.zeros((LANES - 8, LANES), F32)
    key = [jnp.concatenate([k, pad], 0).astype(BF16) for k in key]
    value = [jnp.concatenate([v, pad], 0) for v in (value[:, :LANES], value[:, LANES:])]
    own = sum(matmul_t(q, k) for q, k in zip(query, key))
    for j, part in enumerate(attend([own], [value], [table_ref[SEEN_AT : SEEN_AT + 16] > 0.5])):
        own_ref[j] = part
    anchor = table_ref[ANCHOR_AT : ANCHOR_AT + 1]
    nope_gain = table_ref[GAIN_AT : GAIN_AT + NOPE]
    rope_gain = table_ref[GAIN_AT + NOPE : GAIN_AT + QK]
    products, values, seen = [], [], []
    for k, block_ref in enumerate(block_refs):
        source = lax.rem(lax.axis_index("y") + SEQS - k, SEQS)
        start = (lax.axis_index("z") * SEQS + source) * LANES
        scales = [block_ref[SCALE_AT + h : SCALE_AT + h + 1] for h in range(HEADS)]
        rope = block_ref[TURN_AT : TURN_AT + ROPE]
        keys = [
            block_ref[NOPE * h : NOPE * h + NOPE] * scales[h] * nope_gain for h in range(HEADS)
        ] + [rope * scales[h] * rope_gain for h in range(HEADS)]
        key = jnp.concatenate(keys, 0).astype(BF16)
        products.append(sum(matmul(q, key[LANES * j : LANES * j + LANES]) for j, q in enumerate(query)))
        values.append([block_ref[VALUE_AT + LANES * j : VALUE_AT + LANES * j + LANES] for j in range(2)])
        seen.append((lanes_of((16, LANES)) + start).astype(F32) < anchor)
    packed = attend(products, values, seen)
    for k in range(out_ref.shape[0]):
        for j, part in enumerate(packed):
            out_ref[k, j] = part


def merge_body(in_ref, own_ref, fresh_ref, *refs):
    block_refs, out_ref = refs[:-1], refs[-1]
    y = lax.axis_index("y")
    share = lax.axis_index("x") * lax.axis_size("c") + lax.axis_index("c")
    parts = [[in_ref[k, j] for j in range(3)] for k in range(in_ref.shape[0])]
    parts.append([own_ref[j] for j in range(3)])
    peak = functools.reduce(jnp.maximum, [stats for _, _, stats in parts])
    first = second = total = 0.0
    for first_part, second_part, stats in parts:
        scale = jnp.exp(stats - peak)
        total = total + pltpu.roll(stats, LANES - HEADS, 1) * scale
        first = first + first_part * half_pick(scale[:, 0:1], scale[:, 1:2])
        second = second + second_part * half_pick(scale[:, 2:3], scale[:, 3:4])
    first = first / half_pick(total[:, 0:1], total[:, 1:2])
    second = second / half_pick(total[:, 2:3], total[:, 3:4])
    pad = jnp.zeros((4, LANES), F32)
    first = jnp.concatenate([first, pad], 0).astype(BF16)
    second = jnp.concatenate([second, pad], 0).astype(BF16)
    sums = [jnp.zeros((8, LANES), F32) for _ in range(SEQS)]
    for k, block_ref in enumerate(block_refs):
        weight = block_ref[WEIGHT_AT : WEIGHT_AT + LANES].astype(BF16)
        low = matmul_t(first, weight) + pltpu.roll(matmul_t(second, weight), NOPE, 1)
        both = half_pick(low, pltpu.roll(low, NOPE, 1))
        place = lax.rem(y + SEQS - k, SEQS)
        sums = [jnp.where(place == j, both, sums[j]) for j in range(SEQS)]
    packed = (half_pick(sums[0], sums[1])[0:4], half_pick(sums[2], sums[3])[0:4], fresh_ref[share])
    for k in range(out_ref.shape[0]):
        for j, part in enumerate(packed):
            out_ref[k, j] = part


def gather_body(in_ref, own_ref, square_ref, latent_ref):
    y = lax.axis_index("y")
    peers = in_ref.shape[0] // SEQS
    lane = lanes_of((PROPS, LANES))
    squares = jnp.zeros((PROPS, LANES), F32)
    for s in range(SEQS):
        first, second = in_ref[peers * s, 0], in_ref[peers * s, 1]
        for t in range(1, peers):
            first = first + in_ref[peers * s + t, 0]
            second = second + in_ref[peers * s + t, 1]
        square = jnp.sum(first * first + second * second, -1, keepdims=True)
        squares = jnp.where(lane == s, square, squares)
        picked = jnp.where(y < 2, first, second)
        own_ref[s] = jnp.where(lax.rem(y, 2) == 0, picked, pltpu.roll(picked, NOPE, 1))
        for t in range(peers):
            latent_ref[s, :, LANES * t : LANES * t + LANES] = in_ref[peers * s + t, 2]
    for k in range(square_ref.shape[0]):
        square_ref[k] = squares


def finish_body(in_ref, own_ref, table_ref, window_ref, fresh_ref, copy_hbm, mixed_ref, out_hbm, patch_ref, sems):
    del copy_hbm
    positions = out_hbm.shape[1]
    begun = table_ref[START_AT : START_AT + 1]
    lane = lanes_of(begun.shape)
    starts = [jnp.sum(jnp.where(lane == s, begun, 0.0)).astype(jnp.int32) for s in range(SEQS)]
    for s, start in enumerate(starts):

        @pl.when((start > -PROPS) & (start < positions))
        def _(s=s, start=start):
            base = window_base(start, positions)
            window = window_ref[s].astype(F32)
            row = rows_of(window.shape) + base
            for p in range(PROPS):
                window = jnp.where(row == start + p, fresh_ref[s, p : p + 1, :], window)
            patch_ref[s] = window.astype(BF16)
            pltpu.make_async_copy(patch_ref.at[s], out_hbm.at[s, pl.ds(base, WINDOW), :], sems.at[s]).start()

    total = in_ref[0]
    for k in range(1, in_ref.shape[0]):
        total = total + in_ref[k]
    gain = table_ref[OUT_AT : OUT_AT + 1, 0:NOPE]
    for s in range(SEQS):
        scale = lax.rsqrt(total[:, s : s + 1] / D + EPS)
        mixed_ref[s] = (own_ref[s, :, :NOPE] * scale * gain).astype(BF16)
    for s, start in enumerate(starts):

        @pl.when((start > -PROPS) & (start < positions))
        def _(s=s, start=start):
            base = window_base(start, positions)
            pltpu.make_async_copy(patch_ref.at[s], out_hbm.at[s, pl.ds(base, WINDOW), :], sems.at[s]).wait()


def swap(parts, axis):
    return lax.all_to_all(parts, axis, split_axis=0, concat_axis=0, tiled=True)


def body(
    tokens,
    parents,
    lengths,
    accepted,
    in_gain,
    w_query,
    w_latent,
    w_rope_key,
    latent_gain,
    query_gain,
    key_gain,
    w_key_up,
    w_value_up,
    w_out,
    out_gain,
    cache_latent,
    cache_rope,
):
    depth, tall = lax.axis_size("z"), lax.axis_size("y")
    plane = lax.axis_size(PLANE)
    inverse = 10000.0 ** (-(np.arange(LANES) % 16).astype(np.float32) / 16)
    inverse = jnp.asarray(inverse.astype(np.float32).reshape(1, LANES))
    rope_cols = jnp.swapaxes(cache_rope, 1, 2)

    loaded = (
        parents,
        lengths,
        accepted,
        tokens,
        in_gain.reshape(1, -1),
        w_query,
        w_latent,
        w_rope_key.T,
        inverse,
        latent_gain.reshape(1, -1),
        query_gain.reshape(1, -1),
        key_gain.reshape(1, -1),
        out_gain.reshape(1, -1),
        w_out.T,
        rope_cols,
        w_key_up,
        w_value_up,
        cache_latent,
    )
    sent, block_0, block_1, block_2, block_3, table, windows, new_rope, kept = kernel(
        start_body,
        [
            ((tall, CHUNKS, PROPS, LANES), F32),
            *[((BLOCK_ROWS, LANES), F32)] * SEQS,
            ((TABLE_ROWS, LANES), F32),
            ((SEQS, WINDOW, 1024), BF16),
            (rope_cols.shape, BF16),
            (cache_latent.shape, BF16),
        ],
        *[pltpu.with_memory_space_constraint(a, pltpu.HBM) for a in loaded],
        specs=[HBM] * len(loaded),
        out_specs=[VMEM] * 8 + [HBM],
        scratch=[
            (pltpu.SMEM if k < 3 else pltpu.VMEM)(a.shape, a.dtype) for k, a in enumerate(loaded)
        ]
        + [pltpu.SemaphoreType.DMA((len(loaded) + 1,))],
        mebibytes=16,
    )
    reduced = swap(sent, "y")
    leaving = [block_1, block_2, block_3]
    moved = {0: block_0}
    for k in (2, 1, 3):
        moved[k] = lax.ppermute(leaving[k - 1], "y", [(i, (i + k) % SEQS) for i in range(SEQS)])
    blocks = [moved[k] for k in range(SEQS)]
    spread = kernel(relay_body, [((depth, CHUNKS, PROPS, LANES), F32)], reduced)
    gathered = swap(spread, "z")
    query, latent_half = kernel(query_body, [((3, 16, LANES), F32), ((4, PROPS, LANES), F32)], gathered, table)
    latent_both = lax.all_gather(latent_half, "c")
    partial, own, fresh = kernel(
        attend_body,
        [((depth, 3, PROPS, LANES), F32), ((3, PROPS, LANES), F32), ((8, PROPS, LANES), F32)],
        latent_both,
        table,
        query,
        w_key_up,
        w_value_up,
        *blocks,
    )
    partials = swap(partial, "z")
    projected = kernel(merge_body, [((plane, 3, PROPS, LANES), F32)], partials, own, fresh, *blocks)
    projections = swap(projected, PLANE)
    own_columns, squares, fresh_all = kernel(
        gather_body,
        [((SEQS, PROPS, LANES), F32), ((depth, PROPS, LANES), F32), ((SEQS, PROPS, 1024), F32)],
        projections,
    )
    square_parts = swap(squares, "z")
    mixed, new_latent = kernel(
        finish_body,
        [((SEQS, PROPS, NOPE), BF16), (cache_latent.shape, BF16)],
        square_parts,
        own_columns,
        table,
        windows,
        fresh_all,
        kept,
        specs=[VMEM] * 5 + [HBM],
        out_specs=[VMEM, HBM],
        scratch=[pltpu.VMEM((SEQS, WINDOW, 1024), BF16), pltpu.SemaphoreType.DMA((SEQS,))],
        aliases={5: 1},
    )
    return (mixed, new_latent, jnp.swapaxes(new_rope, 1, 2))


def solution(mesh):
    kv, tp = mesh.shape["kv"], mesh.shape["tp"]
    finer = Mesh(mesh.devices.reshape(kv // 4, 4, tp // 2, 2), ("z", "y", "x", "c"))
    tp_axes = ("x", "c")
    placed = (
        P(),
        P(),
        P(),
        P(),
        P(),
        P(KV, tp_axes),
        P(KV, None),
        P(),
        P(),
        P(),
        P(),
        P(None, tp_axes),
        P(None, tp_axes),
        P(tp_axes, KV),
        P(KV),
        P(None, KV, None),
        P(None, KV, None),
    )
    return jax.shard_map(
        body,
        mesh=finer,
        in_specs=placed,
        out_specs=(P(None, None, KV), P(None, KV, None), P(None, KV, None)),
        check_vma=False,
    )
```

```python
import functools

import jax
import jax.numpy as jnp
import numpy as np
from jax import lax
from jax.experimental import pallas as pl
from jax.experimental.pallas import tpu as pltpu
from jax.sharding import Mesh
from jax.sharding import PartitionSpec as P


D = 4096
NOPE = 64
ROPE = 32
QK = 96
SEQS = 4
PROPS = 4
HEADS = 4
LANES = 128
EPS = 1e-06
KV = ("z", "y")
PLANE = ("y", "x", "c")
F32 = jnp.float32
BF16 = jnp.bfloat16
HIDDEN = -1e30

VMEM = pl.BlockSpec(memory_space=pltpu.VMEM)
HBM = pl.BlockSpec(memory_space=pltpu.HBM)
CHUNKS = 7
PLANE_FIRST, TALL_FIRST = 21, 2
TURN_AT, SCALE_AT, VALUE_AT, WEIGHT_AT, BLOCK_ROWS = 256, 288, 296, 552, 680
ROPE_AT, COS_AT, A_AT, B_AT, SEEN_AT, ANCHOR_AT = 0, 4, 8, 12, 16, 32
QN_AT, QR_AT, KN_AT, KR_AT, OUT_AT, START_AT, LATENT_AT = 33, 34, 35, 36, 37, 38, 40
GAIN_AT, TABLE_ROWS = 48, 144
WINDOW = 32


def kernel(body, outs, *args, specs=None, out_specs=None, scratch=(), aliases=None, mebibytes=8):
    shapes = [jax.ShapeDtypeStruct(shape, kind) for shape, kind in outs]
    out_specs = list(out_specs) if out_specs else [VMEM] * len(shapes)
    single = len(shapes) == 1
    return pl.pallas_call(
        body,
        out_shape=shapes[0] if single else shapes,
        in_specs=list(specs) if specs else [VMEM] * len(args),
        out_specs=out_specs[0] if single else out_specs,
        scratch_shapes=list(scratch),
        input_output_aliases=aliases or {},
        cost_estimate=pl.CostEstimate(flops=2_000_000, bytes_accessed=1_000_000, transcendentals=0),
        compiler_params=pltpu.CompilerParams(vmem_limit_bytes=mebibytes * 2**20),
    )(*args)


def lanes_of(shape):
    return lax.broadcasted_iota(jnp.int32, shape, len(shape) - 1)


def rows_of(shape):
    return lax.broadcasted_iota(jnp.int32, shape, len(shape) - 2)


def matmul(left, right):
    return lax.dot_general(left, right, (((1,), (0,)), ((), ())), preferred_element_type=F32)


def matmul_t(left, right):
    return lax.dot_general(left, right, (((1,), (1,)), ((), ())), preferred_element_type=F32)


def half_pick(low, high):
    shape = jnp.broadcast_shapes(low.shape, high.shape)
    shape = (*shape[:-1], LANES)
    return jnp.where(lanes_of(shape) < NOPE, low, high)


def quarter_pick(parts):
    shape = (*parts[0].shape[:-1], LANES)
    lane = lanes_of(shape)
    return jnp.where(
        lane < NOPE,
        jnp.where(lane < ROPE, parts[0], parts[1]),
        jnp.where(lane < NOPE + ROPE, parts[2], parts[3]),
    )


def head_scales(first, second, rope_squares):
    lane = lanes_of(first.shape)
    found = []
    for h, part in enumerate((first, first, second, second)):
        inside = lane < NOPE if h % 2 == 0 else lane >= NOPE
        squares = jnp.sum(jnp.where(inside, part * part, 0.0), -1, keepdims=True)
        found.append(lax.rsqrt((squares + rope_squares[h]) / QK + EPS))
    return found


def gains(gain_row):
    nope = gain_row[:, :NOPE]
    rope = gain_row[:, NOPE:QK]
    return jnp.concatenate([nope, nope], 1), jnp.concatenate([rope] * 4, 1)


def keys_of(nope, rope_tiled, nope_gain, rope_gain):
    first, second = nope[:, :LANES], nope[:, LANES:]
    lane = lanes_of(rope_tiled.shape)
    rope_sum = jnp.sum(jnp.where(lane < ROPE, rope_tiled * rope_tiled, 0.0), -1, keepdims=True)
    scales = head_scales(first, second, [rope_sum] * 4)
    return (
        first * half_pick(scales[0], scales[1]) * nope_gain,
        second * half_pick(scales[2], scales[3]) * nope_gain,
        rope_tiled * quarter_pick(scales) * rope_gain,
    )


def attend(products, values, seen):
    scale = QK ** (-0.5)
    scores = [jnp.where(v, p * scale, HIDDEN) for p, v in zip(products, seen)]
    peak = functools.reduce(jnp.maximum, [jnp.max(s, -1, keepdims=True) for s in scores])
    weights = [jnp.where(v, jnp.exp(s - peak), 0.0) for s, v in zip(scores, seen)]
    total = sum(jnp.sum(w, -1, keepdims=True) for w in weights)
    sums = [0.0, 0.0]
    for weight, value in zip(weights, values):
        low = weight.astype(BF16)
        for j, part in enumerate(value):
            high_part = part.astype(BF16)
            rest = (part - high_part.astype(F32)).astype(BF16)
            sums[j] = sums[j] + matmul(low, high_part) + matmul(low, rest)
    first = half_pick(sums[0][0:4], sums[0][4:8])
    second = half_pick(sums[1][8:12], sums[1][12:16])
    lane = lanes_of((PROPS, LANES))
    stats = jnp.zeros((PROPS, LANES), F32)
    for h in range(HEADS):
        stats = jnp.where(lane == h, peak[4 * h : 4 * h + 4], stats)
        stats = jnp.where(lane == HEADS + h, total[4 * h : 4 * h + 4], stats)
    return first, second, stats


def sine_cosine(angle):
    turns = jnp.floor(angle * (2.0 / np.pi) + 0.5)
    rest = ((angle - turns * 1.5703125) - turns * 4.837512969970703125e-4) - turns * 7.549789954891882e-8
    square = rest * rest
    sine = rest + rest * square * (
        -1.6666654611e-1 + square * (8.3321608736e-3 + square * -1.9515295891e-4)
    )
    cosine = (
        1.0
        - 0.5 * square
        + square
        * square
        * (4.166664568298827e-2 + square * (-1.388731625493765e-3 + square * 2.443315711809948e-5))
    )
    quadrant = turns - 4.0 * jnp.floor(turns * 0.25)
    odd = (quadrant == 1.0) | (quadrant == 3.0)
    sine_out = jnp.where(odd, cosine, sine)
    cosine_out = jnp.where(odd, sine, cosine)
    sine_out = jnp.where(quadrant >= 2.0, -sine_out, sine_out)
    cosine_out = jnp.where((quadrant == 1.0) | (quadrant == 2.0), -cosine_out, cosine_out)
    return sine_out, cosine_out


def turn(rope_tiled, cosine, sine_a, sine_b):
    return (
        rope_tiled * cosine
        + pltpu.roll(rope_tiled, LANES - 16, 1) * sine_a
        + pltpu.roll(rope_tiled, 16, 1) * sine_b
    )


def ancestors(parents_ref, s):
    masks = []
    for i in range(PROPS):
        mask = jnp.int32(1 << i)
        if i:
            parent = parents_ref[s, i]
            for j in range(i):
                mask = mask + jnp.where(parent == j, masks[j], 0)
        masks.append(mask)
    return masks


def bits(mask):
    return sum((mask >> j) & 1 for j in range(PROPS))


def load(sources, targets, sems):
    copies = [pltpu.make_async_copy(a, b, sems.at[k]) for k, (a, b) in enumerate(zip(sources, targets))]
    for copy in copies:
        copy.start()
    return copies


def start_body(*refs):
    sources, refs = refs[:9], refs[9:]
    (out_ref, *block_refs), refs = refs[:5], refs[5:]
    targets, (nope_ref, value_ref, sems) = refs[:9], refs[9:]
    tok_ref, gain_ref, wq_ref, wl_ref, wo_ref, rope_ref, wk_ref, wv_ref, cache_ref = targets
    copies = load(sources, targets, sems)
    for copy in copies[:4]:
        copy.wait()
    y = lax.axis_index("y")
    kv = lax.axis_index("z") * lax.axis_size("y") + y
    rows = wq_ref.shape[0]
    width = max(rows, LANES)
    per = width // rows
    base = pl.multiple_of((kv // per) * width, LANES)
    positions = cache_ref.shape[1]

    parts = []
    for s in range(SEQS):
        tok = tok_ref[s].astype(F32)
        scale = lax.rsqrt(jnp.sum(tok * tok, -1, keepdims=True) / D + EPS)
        piece = tok_ref[s, :, pl.ds(base, width)].astype(F32)
        parts.append(piece * scale * gain_ref[:, pl.ds(base, width)])
    part = jnp.concatenate(parts, 0)
    if per > 1:
        part = jnp.where(lanes_of(part.shape) // rows == kv % per, part, 0.0)
    part = part.astype(BF16)
    half = wl_ref.shape[1] // 2
    wl = wl_ref[:, pl.ds(pl.multiple_of(lax.axis_index("c") * half, LANES), half)]
    query = matmul(part, jnp.concatenate([wq_ref[...]] * per, 0))
    latent = matmul(part, jnp.concatenate([wl] * per, 0))
    nope = [query[:, QK * h : QK * h + NOPE] for h in range(HEADS)]
    rope = [query[:, QK * h + NOPE : QK * h + QK] for h in range(HEADS)]
    chunks = [
        jnp.concatenate(nope[:2], 1),
        jnp.concatenate(nope[2:], 1),
        jnp.concatenate(rope, 1),
    ] + [latent[:, LANES * k : LANES * k + LANES] for k in range(half // LANES)]
    for s in range(SEQS):
        for k, chunk in enumerate(chunks):
            out_ref[(s - TALL_FIRST) % SEQS, k] = chunk[4 * s : 4 * s + 4]

    for copy in copies[4:]:
        copy.wait()
    whole = cache_ref[...].reshape(SEQS * positions, cache_ref.shape[2])
    nope_ref[...] = matmul(whole, wk_ref[...])
    value_ref[...] = matmul(whole, wv_ref[...])
    weights = wo_ref[...].astype(F32)
    for k, block_ref in enumerate(block_refs):
        s = lax.rem(y + k, SEQS)
        at = pl.ds(pl.multiple_of(s * positions, positions), positions)
        old = rope_ref[s].astype(F32)
        old_sum = jnp.sum(old * old, 0, keepdims=True)
        block_ref[TURN_AT : TURN_AT + ROPE] = old
        for j in range(2):
            lanes = slice(LANES * j, LANES * j + LANES)
            flat = nope_ref[at, lanes].T
            block_ref[lanes] = flat
            block_ref[VALUE_AT + LANES * j : VALUE_AT + LANES * j + LANES] = value_ref[at, lanes]
            for i in range(2):
                dims = flat[NOPE * i : NOPE * i + NOPE]
                squares = jnp.sum(dims * dims, 0, keepdims=True) + old_sum
                h = SCALE_AT + 2 * j + i
                block_ref[h : h + 1] = lax.rsqrt(squares / QK + EPS)
        block_ref[SCALE_AT + 4 : SCALE_AT + 8] = jnp.zeros((4, LANES), F32)
        block_ref[WEIGHT_AT : WEIGHT_AT + 64] = weights[:, :LANES]
        block_ref[WEIGHT_AT + 64 : WEIGHT_AT + 128] = weights[:, LANES:]


def aside_body(*refs):
    sources, refs = refs[:13], refs[13:]
    (table_ref, window_ref, rope_out_ref, copy_hbm), refs = refs[:4], refs[4:]
    targets, sems = refs[:13], refs[13]
    (
        parents_ref, lengths_ref, accepted_ref, tok_ref, gain_ref, wr_ref,
        inverse_ref, lgain_ref, qgain_ref, kgain_ref, ogain_ref, rope_ref, cache_ref,
    ) = targets
    copies = load(sources, targets, sems)
    for copy in copies:
        copy.wait()
    kept = pltpu.make_async_copy(cache_ref, copy_hbm, sems.at[len(copies)])
    kept.start()
    y = lax.axis_index("y")
    kv = lax.axis_index("z") * lax.axis_size("y") + y
    positions = cache_ref.shape[1]
    normed = []
    for s in range(SEQS):
        tok = tok_ref[s].astype(F32)
        scale = lax.rsqrt(jnp.sum(tok * tok, -1, keepdims=True) / D + EPS)
        normed.append(tok * scale * gain_ref[...])

    row = rows_of((16, LANES))
    place = jnp.zeros((16, LANES), F32)
    starts = []
    for s in range(SEQS):
        anchor = lengths_ref[s] + accepted_ref[s]
        starts.append(anchor - kv * positions)
        for i, mask in enumerate(ancestors(parents_ref, s)):
            place = jnp.where(row == 4 * s + i, (anchor + bits(mask) - 1).astype(F32), place)
    raw = matmul_t(jnp.concatenate(normed, 0).astype(BF16), wr_ref[...])
    raw = jnp.concatenate([raw] * 4, 1)
    sine, cosine = sine_cosine(place * inverse_ref[...])
    early = lanes_of((16, LANES)) % ROPE < 16
    sine_a = jnp.where(early, -sine, 0.0)
    sine_b = jnp.where(early, 0.0, sine)
    fresh = turn(raw, cosine, sine_a, sine_b)
    for at, full in ((ROPE_AT, fresh), (COS_AT, cosine), (A_AT, sine_a), (B_AT, sine_b)):
        own = full[0:4]
        for s in range(1, SEQS):
            own = jnp.where(y == s, full[4 * s : 4 * s + 4], own)
        table_ref[at : at + 4] = own
    masks = ancestors(parents_ref, y)
    prop, lane = row % PROPS, lanes_of((16, LANES))
    seen = jnp.zeros((16, LANES), jnp.int32)
    for i in range(PROPS):
        for j in range(i + 1):
            seen = jnp.where((prop == i) & (lane == j), (masks[i] >> j) & 1, seen)
    table_ref[SEEN_AT : SEEN_AT + 16] = seen.astype(F32)
    anchor = (lengths_ref[y] + accepted_ref[y]).astype(F32)
    table_ref[ANCHOR_AT : ANCHOR_AT + 1] = jnp.zeros((1, LANES), F32) + anchor
    nope_gain, rope_gain = gains(kgain_ref[...])
    table_ref[KN_AT : KN_AT + 1], table_ref[KR_AT : KR_AT + 1] = nope_gain, rope_gain
    table_ref[QN_AT : QN_AT + 1], table_ref[QR_AT : QR_AT + 1] = gains(qgain_ref[...])
    table_ref[OUT_AT : OUT_AT + 1] = jnp.concatenate([ogain_ref[...]] * (LANES // ogain_ref.shape[1]), 1)
    spot = lanes_of((2, LANES))
    begun = jnp.zeros((2, LANES), F32)
    for s in range(SEQS):
        begun = jnp.where(spot == s, starts[s].astype(F32), begun)
    table_ref[START_AT : START_AT + 2] = begun
    for k in range(8):
        table_ref[LATENT_AT + k : LATENT_AT + k + 1] = lgain_ref[:, LANES * k : LANES * k + LANES]
    tall_gain = jnp.concatenate([nope_gain, rope_gain, jnp.zeros((6, LANES), F32)], 0)
    tall_gain = jnp.concatenate([tall_gain] * (LANES // 8), 0).T
    table_ref[GAIN_AT : GAIN_AT + NOPE] = jnp.zeros((NOPE, LANES), F32) + tall_gain[:NOPE, 0:1]
    table_ref[GAIN_AT + NOPE : GAIN_AT + QK] = jnp.zeros((ROPE, LANES), F32) + tall_gain[:ROPE, 1:2]
    flipped = jnp.concatenate([fresh, jnp.zeros((LANES - 16, LANES), F32)], 0).T[:ROPE]

    for s in range(SEQS):
        old = rope_ref[s].astype(F32)
        spot = lanes_of(old.shape)
        for p in range(PROPS):
            old = jnp.where(spot == starts[s] + p, flipped[:, 4 * s + p : 4 * s + p + 1], old)
        rope_out_ref[s] = old.astype(BF16)
        window_ref[s] = cache_ref[s, pl.ds(window_base(starts[s], positions), WINDOW), :]
    kept.wait()


def window_base(start, positions):
    return pl.multiple_of(jnp.clip(start // 16, 0, positions // 16 - WINDOW // 16) * 16, 16)


def relay_body(in_ref, out_ref):
    total = in_ref[0]
    for k in range(1, in_ref.shape[0]):
        total = total + in_ref[k]
    for k in range(out_ref.shape[0]):
        out_ref[k] = total


def query_body(in_ref, table_ref, query_ref, latent_ref):
    total = in_ref[0]
    for k in range(1, in_ref.shape[0]):
        total = total + in_ref[k]
    first, second = total[0], total[1]
    rope = turn(
        total[2],
        table_ref[COS_AT : COS_AT + 4],
        table_ref[A_AT : A_AT + 4],
        table_ref[B_AT : B_AT + 4],
    )
    lane = lanes_of(rope.shape)
    sums = [
        jnp.sum(jnp.where(lane // ROPE == h, rope * rope, 0.0), -1, keepdims=True)
        for h in range(HEADS)
    ]
    scales = head_scales(first, second, sums)
    nope_gain, rope_gain = table_ref[QN_AT : QN_AT + 1], table_ref[QR_AT : QR_AT + 1]
    first = first * half_pick(scales[0], scales[1]) * nope_gain
    second = second * half_pick(scales[2], scales[3]) * nope_gain
    rope = rope * quarter_pick(scales) * rope_gain
    for h in range(HEADS):
        inside = (lane < NOPE) if h % 2 == 0 else (lane >= NOPE)
        empty = jnp.zeros_like(first)
        query_ref[0, 4 * h : 4 * h + 4] = jnp.where(inside, first, 0.0) if h < 2 else empty
        query_ref[1, 4 * h : 4 * h + 4] = jnp.where(inside, second, 0.0) if h >= 2 else empty
        query_ref[2, 4 * h : 4 * h + 4] = jnp.where(lane // ROPE == h, rope, 0.0)
    latent_ref[...] = total[3:CHUNKS]


def own_body(latent_ref, table_ref, query_ref, wk_ref, wv_ref, own_ref, fresh_ref):
    query = [query_ref[j].astype(BF16) for j in range(3)]
    pieces = [latent_ref[c, k] for c in range(2) for k in range(4)]
    squares = sum(jnp.sum(piece * piece, -1, keepdims=True) for piece in pieces)
    scale = lax.rsqrt(squares / (8 * LANES) + EPS)
    pieces = [p * scale * table_ref[LATENT_AT + k : LATENT_AT + k + 1] for k, p in enumerate(pieces)]
    for k, piece in enumerate(pieces):
        fresh_ref[k] = piece
    fresh = jnp.concatenate(pieces, 1)
    low = jnp.concatenate([fresh, jnp.zeros_like(fresh)], 0).astype(BF16)
    value = matmul(low, wv_ref[...])
    rope = table_ref[ROPE_AT : ROPE_AT + 4].astype(BF16).astype(F32)
    tiled = jnp.concatenate([rope, jnp.zeros_like(rope)], 0)
    key = keys_of(
        matmul(low, wk_ref[...]), tiled, table_ref[KN_AT : KN_AT + 1], table_ref[KR_AT : KR_AT + 1]
    )
    pad = jnp.zeros((LANES - 8, LANES), F32)
    key = [jnp.concatenate([k, pad], 0).astype(BF16) for k in key]
    value = [jnp.concatenate([v, pad], 0) for v in (value[:, :LANES], value[:, LANES:])]
    own = sum(matmul_t(q, k) for q, k in zip(query, key))
    for j, part in enumerate(attend([own], [value], [table_ref[SEEN_AT : SEEN_AT + 16] > 0.5])):
        own_ref[j] = part


def attend_body(table_ref, query_ref, *refs):
    block_refs, out_ref = refs[:-1], refs[-1]
    query = [query_ref[j].astype(BF16) for j in range(3)]
    anchor = table_ref[ANCHOR_AT : ANCHOR_AT + 1]
    nope_gain = table_ref[GAIN_AT : GAIN_AT + NOPE]
    rope_gain = table_ref[GAIN_AT + NOPE : GAIN_AT + QK]
    products, values, seen = [], [], []
    for k, block_ref in enumerate(block_refs):
        source = lax.rem(lax.axis_index("y") + SEQS - k, SEQS)
        start = (lax.axis_index("z") * SEQS + source) * LANES
        scales = [block_ref[SCALE_AT + h : SCALE_AT + h + 1] for h in range(HEADS)]
        rope = block_ref[TURN_AT : TURN_AT + ROPE]
        keys = [
            block_ref[NOPE * h : NOPE * h + NOPE] * scales[h] * nope_gain for h in range(HEADS)
        ] + [rope * scales[h] * rope_gain for h in range(HEADS)]
        key = jnp.concatenate(keys, 0).astype(BF16)
        products.append(sum(matmul(q, key[LANES * j : LANES * j + LANES]) for j, q in enumerate(query)))
        values.append([block_ref[VALUE_AT + LANES * j : VALUE_AT + LANES * j + LANES] for j in range(2)])
        seen.append((lanes_of((16, LANES)) + start).astype(F32) < anchor)
    packed = attend(products, values, seen)
    for k in range(out_ref.shape[0]):
        for j, part in enumerate(packed):
            out_ref[k, j] = part


def merge_body(in_ref, own_ref, fresh_ref, *refs):
    block_refs, out_ref = refs[:-1], refs[-1]
    y = lax.axis_index("y")
    share = lax.axis_index("x") * lax.axis_size("c") + lax.axis_index("c")
    parts = [[in_ref[k, j] for j in range(3)] for k in range(in_ref.shape[0])]
    parts.append([own_ref[j] for j in range(3)])
    peak = functools.reduce(jnp.maximum, [stats for _, _, stats in parts])
    first = second = total = 0.0
    for first_part, second_part, stats in parts:
        scale = jnp.exp(stats - peak)
        total = total + pltpu.roll(stats, LANES - HEADS, 1) * scale
        first = first + first_part * half_pick(scale[:, 0:1], scale[:, 1:2])
        second = second + second_part * half_pick(scale[:, 2:3], scale[:, 3:4])
    first = first / half_pick(total[:, 0:1], total[:, 1:2])
    second = second / half_pick(total[:, 2:3], total[:, 3:4])
    pad = jnp.zeros((4, LANES), F32)
    first = jnp.concatenate([first, pad], 0).astype(BF16)
    second = jnp.concatenate([second, pad], 0).astype(BF16)
    sums = [jnp.zeros((8, LANES), F32) for _ in range(SEQS)]
    for k, block_ref in enumerate(block_refs):
        weight = block_ref[WEIGHT_AT : WEIGHT_AT + LANES].astype(BF16)
        low = matmul_t(first, weight) + pltpu.roll(matmul_t(second, weight), NOPE, 1)
        both = half_pick(low, pltpu.roll(low, NOPE, 1))
        place = lax.rem(y + SEQS - k, SEQS)
        sums = [jnp.where(place == j, both, sums[j]) for j in range(SEQS)]
    packed = (half_pick(sums[0], sums[1])[0:4], half_pick(sums[2], sums[3])[0:4], fresh_ref[share])
    for k in range(out_ref.shape[0]):
        for j, part in enumerate(packed):
            out_ref[k, j] = part


def gather_body(whole_ref, own_ref, square_ref, latent_ref):
    y = lax.axis_index("y")
    size = whole_ref.shape[0]
    peers = size // SEQS
    in_ref = [whole_ref.at[(k - PLANE_FIRST) % size] for k in range(size)]
    lane = lanes_of((PROPS, LANES))
    squares = jnp.zeros((PROPS, LANES), F32)
    for s in range(SEQS):
        first, second = in_ref[peers * s][0], in_ref[peers * s][1]
        for t in range(1, peers):
            first = first + in_ref[peers * s + t][0]
            second = second + in_ref[peers * s + t][1]
        square = jnp.sum(first * first + second * second, -1, keepdims=True)
        squares = squares + jnp.where(lane == PROPS * s + rows_of(lane.shape), square, 0.0)
        picked = jnp.where(y < 2, first, second)
        own_ref[s] = jnp.where(lax.rem(y, 2) == 0, picked, pltpu.roll(picked, NOPE, 1))
        for t in range(peers):
            latent_ref[s, :, LANES * t : LANES * t + LANES] = in_ref[peers * s + t][2]
    squares = jnp.sum(squares, 0, keepdims=True)
    for k in range(square_ref.shape[0]):
        square_ref[k] = squares


def finish_body(in_ref, own_ref, table_ref, window_ref, fresh_ref, copy_hbm, mixed_ref, out_hbm, patch_ref, sems):
    del copy_hbm
    positions = out_hbm.shape[1]
    begun = table_ref[START_AT : START_AT + 1]
    lane = lanes_of(begun.shape)
    starts = [jnp.sum(jnp.where(lane == s, begun, 0.0)).astype(jnp.int32) for s in range(SEQS)]
    for s, start in enumerate(starts):

        @pl.when((start > -PROPS) & (start < positions))
        def _(s=s, start=start):
            base = window_base(start, positions)
            window = window_ref[s].astype(F32)
            row = rows_of(window.shape) + base
            for p in range(PROPS):
                window = jnp.where(row == start + p, fresh_ref[s, p : p + 1, :], window)
            patch_ref[s] = window.astype(BF16)
            pltpu.make_async_copy(patch_ref.at[s], out_hbm.at[s, pl.ds(base, WINDOW), :], sems.at[s]).start()

    total = in_ref[0]
    for k in range(1, in_ref.shape[0]):
        total = total + in_ref[k]
    gain = table_ref[OUT_AT : OUT_AT + 1, 0:NOPE]
    spread = (PROPS, LANES)
    for s in range(SEQS):
        square = jnp.where(lanes_of(spread) == PROPS * s + rows_of(spread), total, 0.0)
        scale = lax.rsqrt(jnp.sum(square, -1, keepdims=True) / D + EPS)
        mixed_ref[s] = (own_ref[s, :, :NOPE] * scale * gain).astype(BF16)
    for s, start in enumerate(starts):

        @pl.when((start > -PROPS) & (start < positions))
        def _(s=s, start=start):
            base = window_base(start, positions)
            pltpu.make_async_copy(patch_ref.at[s], out_hbm.at[s, pl.ds(base, WINDOW), :], sems.at[s]).wait()


def swap(parts, axis, first=0):
    groups = None
    if first:
        size = lax.axis_size(axis)
        groups = [[(first + k) % size for k in range(size)]]
    return lax.all_to_all(
        parts, axis, split_axis=0, concat_axis=0, tiled=True, axis_index_groups=groups
    )


def body(
    tokens,
    parents,
    lengths,
    accepted,
    in_gain,
    w_query,
    w_latent,
    w_rope_key,
    latent_gain,
    query_gain,
    key_gain,
    w_key_up,
    w_value_up,
    w_out,
    out_gain,
    cache_latent,
    cache_rope,
):
    depth, tall = lax.axis_size("z"), lax.axis_size("y")
    plane = lax.axis_size(PLANE)
    inverse = 10000.0 ** (-(np.arange(LANES) % 16).astype(np.float32) / 16)
    inverse = jnp.asarray(inverse.astype(np.float32).reshape(1, LANES))
    rope_cols = jnp.swapaxes(cache_rope, 1, 2)

    in_row = in_gain.reshape(1, -1)

    def from_hbm(body, outs, out_specs, args, extra):
        args = [pltpu.with_memory_space_constraint(a, pltpu.HBM) for a in args]
        scratch = [
            (pltpu.SMEM if a.dtype == jnp.int32 else pltpu.VMEM)(a.shape, a.dtype) for a in args
        ]
        return kernel(
            body,
            outs,
            *args,
            specs=[HBM] * len(args),
            out_specs=out_specs,
            scratch=[*scratch, *extra, pltpu.SemaphoreType.DMA((len(args) + 1,))],
            mebibytes=16,
        )

    sent, block_0, block_1, block_2, block_3 = from_hbm(
        start_body,
        [((tall, CHUNKS, PROPS, LANES), F32), *[((BLOCK_ROWS, LANES), F32)] * SEQS],
        [VMEM] * 5,
        (tokens, in_row, w_query, w_latent, w_out.T, rope_cols, w_key_up, w_value_up, cache_latent),
        [pltpu.VMEM((SEQS * cache_latent.shape[1], 256), F32)] * 2,
    )
    table, windows, new_rope, kept = from_hbm(
        aside_body,
        [((TABLE_ROWS, LANES), F32), ((SEQS, WINDOW, 1024), BF16), (rope_cols.shape, BF16), (cache_latent.shape, BF16)],
        [VMEM] * 3 + [HBM],
        (
            parents,
            lengths,
            accepted,
            tokens,
            in_row,
            w_rope_key.T,
            inverse,
            latent_gain.reshape(1, -1),
            query_gain.reshape(1, -1),
            key_gain.reshape(1, -1),
            out_gain.reshape(1, -1),
            rope_cols,
            cache_latent,
        ),
        [],
    )
    reduced = swap(sent, "y", TALL_FIRST)
    leaving = [block_1, block_2, block_3]
    moved = {0: block_0}
    for k in (2, 1, 3):
        moved[k] = lax.ppermute(leaving[k - 1], "y", [(i, (i + k) % SEQS) for i in range(SEQS)])
    blocks = [moved[k] for k in range(SEQS)]
    spread = kernel(relay_body, [((depth, CHUNKS, PROPS, LANES), F32)], reduced)
    gathered = swap(spread, "z", depth // 2)
    query, latent_half = kernel(query_body, [((3, 16, LANES), F32), ((4, PROPS, LANES), F32)], gathered, table)
    latent_both = lax.all_gather(latent_half, "c")
    own, fresh = kernel(
        own_body, [((3, PROPS, LANES), F32), ((8, PROPS, LANES), F32)], latent_both, table, query, w_key_up, w_value_up
    )
    partial = kernel(attend_body, [((depth, 3, PROPS, LANES), F32)], table, query, *blocks)
    partials = swap(partial, "z", depth // 2)
    projected = kernel(merge_body, [((plane, 3, PROPS, LANES), F32)], partials, own, fresh, *blocks)
    projections = swap(projected, PLANE, PLANE_FIRST)
    own_columns, squares, fresh_all = kernel(
        gather_body, [((SEQS, PROPS, LANES), F32), ((depth, 1, LANES), F32), ((SEQS, PROPS, 1024), F32)], projections
    )
    square_parts = swap(squares, "z", depth // 2)
    mixed, new_latent = kernel(
        finish_body,
        [((SEQS, PROPS, NOPE), BF16), (cache_latent.shape, BF16)],
        square_parts,
        own_columns,
        table,
        windows,
        fresh_all,
        kept,
        specs=[VMEM] * 5 + [HBM],
        out_specs=[VMEM, HBM],
        scratch=[pltpu.VMEM((SEQS, WINDOW, 1024), BF16), pltpu.SemaphoreType.DMA((SEQS,))],
        aliases={5: 1},
    )
    return (mixed, new_latent, jnp.swapaxes(new_rope, 1, 2))


def solution(mesh):
    kv, tp = mesh.shape["kv"], mesh.shape["tp"]
    finer = Mesh(mesh.devices.reshape(kv // 4, 4, tp // 2, 2), ("z", "y", "x", "c"))
    tp_axes = ("x", "c")
    placed = (
        P(),
        P(),
        P(),
        P(),
        P(),
        P(KV, tp_axes),
        P(KV, None),
        P(),
        P(),
        P(),
        P(),
        P(None, tp_axes),
        P(None, tp_axes),
        P(tp_axes, KV),
        P(KV),
        P(None, KV, None),
        P(None, KV, None),
    )
    return jax.shard_map(
        body,
        mesh=finer,
        in_specs=placed,
        out_specs=(P(None, None, KV), P(None, KV, None), P(None, KV, None)),
        check_vma=False,
    )
```

```python
import functools

import jax
import jax.numpy as jnp
import numpy as np
from jax import lax
from jax.experimental import pallas as pl
from jax.experimental.pallas import tpu as pltpu
from jax.sharding import Mesh
from jax.sharding import PartitionSpec as P


D = 4096
NOPE = 64
ROPE = 32
QK = 96
SEQS = 4
PROPS = 4
HEADS = 4
LANES = 128
EPS = 1e-06
KV = ("z", "y")
PLANE = ("y", "x", "c")
F32 = jnp.float32
BF16 = jnp.bfloat16
HIDDEN = -1e30

VMEM = pl.BlockSpec(memory_space=pltpu.VMEM)
HBM = pl.BlockSpec(memory_space=pltpu.HBM)
CHUNKS = 7
PLANE_FIRST, TALL_FIRST = 21, 2
TURN_AT, SCALE_AT, VALUE_AT, WEIGHT_AT, BLOCK_ROWS = 256, 288, 296, 552, 680
ROPE_AT, COS_AT, A_AT, B_AT, SEEN_AT, ANCHOR_AT = 0, 4, 8, 12, 16, 32
QN_AT, QR_AT, KN_AT, KR_AT, OUT_AT, START_AT, LATENT_AT = 33, 34, 35, 36, 37, 38, 40
GAIN_AT, TABLE_ROWS = 48, 144
WINDOW = 32


def kernel(body, outs, *args, specs=None, out_specs=None, scratch=(), aliases=None, mebibytes=8):
    shapes = [jax.ShapeDtypeStruct(shape, kind) for shape, kind in outs]
    out_specs = list(out_specs) if out_specs else [VMEM] * len(shapes)
    single = len(shapes) == 1
    return pl.pallas_call(
        body,
        out_shape=shapes[0] if single else shapes,
        in_specs=list(specs) if specs else [VMEM] * len(args),
        out_specs=out_specs[0] if single else out_specs,
        scratch_shapes=list(scratch),
        input_output_aliases=aliases or {},
        cost_estimate=pl.CostEstimate(flops=2_000_000, bytes_accessed=1_000_000, transcendentals=0),
        compiler_params=pltpu.CompilerParams(vmem_limit_bytes=mebibytes * 2**20),
    )(*args)


def lanes_of(shape):
    return lax.broadcasted_iota(jnp.int32, shape, len(shape) - 1)


def rows_of(shape):
    return lax.broadcasted_iota(jnp.int32, shape, len(shape) - 2)


def matmul(left, right):
    return lax.dot_general(left, right, (((1,), (0,)), ((), ())), preferred_element_type=F32)


def matmul_t(left, right):
    return lax.dot_general(left, right, (((1,), (1,)), ((), ())), preferred_element_type=F32)


def half_pick(low, high):
    shape = jnp.broadcast_shapes(low.shape, high.shape)
    shape = (*shape[:-1], LANES)
    return jnp.where(lanes_of(shape) < NOPE, low, high)


def quarter_pick(parts):
    shape = (*parts[0].shape[:-1], LANES)
    lane = lanes_of(shape)
    return jnp.where(
        lane < NOPE,
        jnp.where(lane < ROPE, parts[0], parts[1]),
        jnp.where(lane < NOPE + ROPE, parts[2], parts[3]),
    )


def head_scales(first, second, rope_squares):
    lane = lanes_of(first.shape)
    found = []
    for h, part in enumerate((first, first, second, second)):
        inside = lane < NOPE if h % 2 == 0 else lane >= NOPE
        squares = jnp.sum(jnp.where(inside, part * part, 0.0), -1, keepdims=True)
        found.append(lax.rsqrt((squares + rope_squares[h]) / QK + EPS))
    return found


def gains(gain_row):
    nope = gain_row[:, :NOPE]
    rope = gain_row[:, NOPE:QK]
    return jnp.concatenate([nope, nope], 1), jnp.concatenate([rope] * 4, 1)


def keys_of(nope, rope_tiled, nope_gain, rope_gain):
    first, second = nope[:, :LANES], nope[:, LANES:]
    lane = lanes_of(rope_tiled.shape)
    rope_sum = jnp.sum(jnp.where(lane < ROPE, rope_tiled * rope_tiled, 0.0), -1, keepdims=True)
    scales = head_scales(first, second, [rope_sum] * 4)
    return (
        first * half_pick(scales[0], scales[1]) * nope_gain,
        second * half_pick(scales[2], scales[3]) * nope_gain,
        rope_tiled * quarter_pick(scales) * rope_gain,
    )


def attend(products, values, seen):
    scale = QK ** (-0.5)
    scores = [jnp.where(v, p * scale, HIDDEN) for p, v in zip(products, seen)]
    peak = functools.reduce(jnp.maximum, [jnp.max(s, -1, keepdims=True) for s in scores])
    weights = [jnp.where(v, jnp.exp(s - peak), 0.0) for s, v in zip(scores, seen)]
    total = sum(jnp.sum(w, -1, keepdims=True) for w in weights)
    sums = [0.0, 0.0]
    for weight, value in zip(weights, values):
        low = weight.astype(BF16)
        for j, part in enumerate(value):
            high_part = part.astype(BF16)
            rest = (part - high_part.astype(F32)).astype(BF16)
            sums[j] = sums[j] + matmul(low, high_part) + matmul(low, rest)
    first = half_pick(sums[0][0:4], sums[0][4:8])
    second = half_pick(sums[1][8:12], sums[1][12:16])
    lane = lanes_of((PROPS, LANES))
    stats = jnp.zeros((PROPS, LANES), F32)
    for h in range(HEADS):
        stats = jnp.where(lane == h, peak[4 * h : 4 * h + 4], stats)
        stats = jnp.where(lane == HEADS + h, total[4 * h : 4 * h + 4], stats)
    return first, second, stats


def sine_cosine(angle):
    turns = jnp.floor(angle * (2.0 / np.pi) + 0.5)
    rest = ((angle - turns * 1.5703125) - turns * 4.837512969970703125e-4) - turns * 7.549789954891882e-8
    square = rest * rest
    sine = rest + rest * square * (
        -1.6666654611e-1 + square * (8.3321608736e-3 + square * -1.9515295891e-4)
    )
    cosine = (
        1.0
        - 0.5 * square
        + square
        * square
        * (4.166664568298827e-2 + square * (-1.388731625493765e-3 + square * 2.443315711809948e-5))
    )
    quadrant = turns - 4.0 * jnp.floor(turns * 0.25)
    odd = (quadrant == 1.0) | (quadrant == 3.0)
    sine_out = jnp.where(odd, cosine, sine)
    cosine_out = jnp.where(odd, sine, cosine)
    sine_out = jnp.where(quadrant >= 2.0, -sine_out, sine_out)
    cosine_out = jnp.where((quadrant == 1.0) | (quadrant == 2.0), -cosine_out, cosine_out)
    return sine_out, cosine_out


def turn(rope_tiled, cosine, sine_a, sine_b):
    return (
        rope_tiled * cosine
        + pltpu.roll(rope_tiled, LANES - 16, 1) * sine_a
        + pltpu.roll(rope_tiled, 16, 1) * sine_b
    )


def ancestors(parents_ref, s):
    masks = []
    for i in range(PROPS):
        mask = jnp.int32(1 << i)
        if i:
            parent = parents_ref[s, i]
            for j in range(i):
                mask = mask + jnp.where(parent == j, masks[j], 0)
        masks.append(mask)
    return masks


def bits(mask):
    return sum((mask >> j) & 1 for j in range(PROPS))


def load(sources, targets, sems):
    copies = [pltpu.make_async_copy(a, b, sems.at[k]) for k, (a, b) in enumerate(zip(sources, targets))]
    for copy in copies:
        copy.start()
    return copies


def start_body(*refs):
    sources, refs = refs[:9], refs[9:]
    (out_hbm, *block_refs), refs = refs[:5], refs[5:]
    targets, (nope_ref, value_ref, out_ref, sems) = refs[:9], refs[9:]
    tok_ref, gain_ref, wq_ref, wl_ref, wo_ref, rope_ref, wk_ref, wv_ref, cache_ref = targets
    copies = load(sources, targets, sems)
    for copy in copies[:4]:
        copy.wait()
    y = lax.axis_index("y")
    kv = lax.axis_index("z") * lax.axis_size("y") + y
    rows = wq_ref.shape[0]
    width = max(rows, LANES)
    per = width // rows
    base = pl.multiple_of((kv // per) * width, LANES)
    positions = cache_ref.shape[1]

    parts = []
    for s in range(SEQS):
        tok = tok_ref[s].astype(F32)
        scale = lax.rsqrt(jnp.sum(tok * tok, -1, keepdims=True) / D + EPS)
        piece = tok_ref[s, :, pl.ds(base, width)].astype(F32)
        parts.append(piece * scale * gain_ref[:, pl.ds(base, width)])
    part = jnp.concatenate(parts, 0)
    if per > 1:
        part = jnp.where(lanes_of(part.shape) // rows == kv % per, part, 0.0)
    part = part.astype(BF16)
    half = wl_ref.shape[1] // 2
    wl = wl_ref[:, pl.ds(pl.multiple_of(lax.axis_index("c") * half, LANES), half)]
    query = matmul(part, jnp.concatenate([wq_ref[...]] * per, 0))
    latent = matmul(part, jnp.concatenate([wl] * per, 0))
    nope = [query[:, QK * h : QK * h + NOPE] for h in range(HEADS)]
    rope = [query[:, QK * h + NOPE : QK * h + QK] for h in range(HEADS)]
    chunks = [
        jnp.concatenate(nope[:2], 1),
        jnp.concatenate(nope[2:], 1),
        jnp.concatenate(rope, 1),
    ] + [latent[:, LANES * k : LANES * k + LANES] for k in range(half // LANES)]
    for s in range(SEQS):
        for k, chunk in enumerate(chunks):
            out_ref[(s - TALL_FIRST) % SEQS, k] = chunk[4 * s : 4 * s + 4]
    leaving = pltpu.make_async_copy(out_ref, out_hbm, sems.at[len(copies)])
    leaving.start()

    for copy in copies[4:]:
        copy.wait()
    whole = cache_ref[...].reshape(SEQS * positions, cache_ref.shape[2])
    nope_ref[...] = matmul(whole, wk_ref[...])
    value_ref[...] = matmul(whole, wv_ref[...])
    weights = wo_ref[...].astype(F32)
    for k, block_ref in enumerate(block_refs):
        s = lax.rem(y + k, SEQS)
        at = pl.ds(pl.multiple_of(s * positions, positions), positions)
        old = rope_ref[s].astype(F32)
        old_sum = jnp.sum(old * old, 0, keepdims=True)
        block_ref[TURN_AT : TURN_AT + ROPE] = old
        for j in range(2):
            lanes = slice(LANES * j, LANES * j + LANES)
            flat = nope_ref[at, lanes].T
            block_ref[lanes] = flat
            block_ref[VALUE_AT + LANES * j : VALUE_AT + LANES * j + LANES] = value_ref[at, lanes]
            for i in range(2):
                dims = flat[NOPE * i : NOPE * i + NOPE]
                squares = jnp.sum(dims * dims, 0, keepdims=True) + old_sum
                h = SCALE_AT + 2 * j + i
                block_ref[h : h + 1] = lax.rsqrt(squares / QK + EPS)
        block_ref[SCALE_AT + 4 : SCALE_AT + 8] = jnp.zeros((4, LANES), F32)
        block_ref[WEIGHT_AT : WEIGHT_AT + 64] = weights[:, :LANES]
        block_ref[WEIGHT_AT + 64 : WEIGHT_AT + 128] = weights[:, LANES:]
    leaving.wait()


def aside_body(*refs):
    sources, refs = refs[:13], refs[13:]
    (table_ref, window_ref, rope_out_ref, copy_hbm), refs = refs[:4], refs[4:]
    targets, sems = refs[:13], refs[13]
    (
        parents_ref, lengths_ref, accepted_ref, tok_ref, gain_ref, wr_ref,
        inverse_ref, lgain_ref, qgain_ref, kgain_ref, ogain_ref, rope_ref, cache_ref,
    ) = targets
    copies = load(sources, targets, sems)
    for copy in copies:
        copy.wait()
    kept = pltpu.make_async_copy(cache_ref, copy_hbm, sems.at[len(copies)])
    kept.start()
    y = lax.axis_index("y")
    kv = lax.axis_index("z") * lax.axis_size("y") + y
    positions = cache_ref.shape[1]
    normed = []
    for s in range(SEQS):
        tok = tok_ref[s].astype(F32)
        scale = lax.rsqrt(jnp.sum(tok * tok, -1, keepdims=True) / D + EPS)
        normed.append(tok * scale * gain_ref[...])

    row = rows_of((16, LANES))
    place = jnp.zeros((16, LANES), F32)
    starts = []
    for s in range(SEQS):
        anchor = lengths_ref[s] + accepted_ref[s]
        starts.append(anchor - kv * positions)
        for i, mask in enumerate(ancestors(parents_ref, s)):
            place = jnp.where(row == 4 * s + i, (anchor + bits(mask) - 1).astype(F32), place)
    raw = matmul_t(jnp.concatenate(normed, 0).astype(BF16), wr_ref[...])
    raw = jnp.concatenate([raw] * 4, 1)
    sine, cosine = sine_cosine(place * inverse_ref[...])
    early = lanes_of((16, LANES)) % ROPE < 16
    sine_a = jnp.where(early, -sine, 0.0)
    sine_b = jnp.where(early, 0.0, sine)
    fresh = turn(raw, cosine, sine_a, sine_b)
    for at, full in ((ROPE_AT, fresh), (COS_AT, cosine), (A_AT, sine_a), (B_AT, sine_b)):
        own = full[0:4]
        for s in range(1, SEQS):
            own = jnp.where(y == s, full[4 * s : 4 * s + 4], own)
        table_ref[at : at + 4] = own
    masks = ancestors(parents_ref, y)
    prop, lane = row % PROPS, lanes_of((16, LANES))
    seen = jnp.zeros((16, LANES), jnp.int32)
    for i in range(PROPS):
        for j in range(i + 1):
            seen = jnp.where((prop == i) & (lane == j), (masks[i] >> j) & 1, seen)
    table_ref[SEEN_AT : SEEN_AT + 16] = seen.astype(F32)
    anchor = (lengths_ref[y] + accepted_ref[y]).astype(F32)
    table_ref[ANCHOR_AT : ANCHOR_AT + 1] = jnp.zeros((1, LANES), F32) + anchor
    nope_gain, rope_gain = gains(kgain_ref[...])
    table_ref[KN_AT : KN_AT + 1], table_ref[KR_AT : KR_AT + 1] = nope_gain, rope_gain
    table_ref[QN_AT : QN_AT + 1], table_ref[QR_AT : QR_AT + 1] = gains(qgain_ref[...])
    table_ref[OUT_AT : OUT_AT + 1] = jnp.concatenate([ogain_ref[...]] * (LANES // ogain_ref.shape[1]), 1)
    spot = lanes_of((2, LANES))
    begun = jnp.zeros((2, LANES), F32)
    for s in range(SEQS):
        begun = jnp.where(spot == s, starts[s].astype(F32), begun)
    table_ref[START_AT : START_AT + 2] = begun
    for k in range(8):
        table_ref[LATENT_AT + k : LATENT_AT + k + 1] = lgain_ref[:, LANES * k : LANES * k + LANES]
    tall_gain = jnp.concatenate([nope_gain, rope_gain, jnp.zeros((6, LANES), F32)], 0)
    tall_gain = jnp.concatenate([tall_gain] * (LANES // 8), 0).T
    table_ref[GAIN_AT : GAIN_AT + NOPE] = jnp.zeros((NOPE, LANES), F32) + tall_gain[:NOPE, 0:1]
    table_ref[GAIN_AT + NOPE : GAIN_AT + QK] = jnp.zeros((ROPE, LANES), F32) + tall_gain[:ROPE, 1:2]
    flipped = jnp.concatenate([fresh, jnp.zeros((LANES - 16, LANES), F32)], 0).T[:ROPE]

    for s in range(SEQS):
        old = rope_ref[s].astype(F32)
        spot = lanes_of(old.shape)
        for p in range(PROPS):
            old = jnp.where(spot == starts[s] + p, flipped[:, 4 * s + p : 4 * s + p + 1], old)
        rope_out_ref[s] = old.astype(BF16)
        window_ref[s] = cache_ref[s, pl.ds(window_base(starts[s], positions), WINDOW), :]
    kept.wait()


def window_base(start, positions):
    return pl.multiple_of(jnp.clip(start // 16, 0, positions // 16 - WINDOW // 16) * 16, 16)


def relay_body(in_ref, out_ref):
    total = in_ref[0]
    for k in range(1, in_ref.shape[0]):
        total = total + in_ref[k]
    for k in range(out_ref.shape[0]):
        out_ref[k] = total


def query_body(in_ref, table_ref, query_ref, latent_ref):
    total = in_ref[0]
    for k in range(1, in_ref.shape[0]):
        total = total + in_ref[k]
    first, second = total[0], total[1]
    rope = turn(
        total[2],
        table_ref[COS_AT : COS_AT + 4],
        table_ref[A_AT : A_AT + 4],
        table_ref[B_AT : B_AT + 4],
    )
    lane = lanes_of(rope.shape)
    sums = [
        jnp.sum(jnp.where(lane // ROPE == h, rope * rope, 0.0), -1, keepdims=True)
        for h in range(HEADS)
    ]
    scales = head_scales(first, second, sums)
    nope_gain, rope_gain = table_ref[QN_AT : QN_AT + 1], table_ref[QR_AT : QR_AT + 1]
    first = first * half_pick(scales[0], scales[1]) * nope_gain
    second = second * half_pick(scales[2], scales[3]) * nope_gain
    rope = rope * quarter_pick(scales) * rope_gain
    for h in range(HEADS):
        inside = (lane < NOPE) if h % 2 == 0 else (lane >= NOPE)
        empty = jnp.zeros_like(first)
        query_ref[0, 4 * h : 4 * h + 4] = jnp.where(inside, first, 0.0) if h < 2 else empty
        query_ref[1, 4 * h : 4 * h + 4] = jnp.where(inside, second, 0.0) if h >= 2 else empty
        query_ref[2, 4 * h : 4 * h + 4] = jnp.where(lane // ROPE == h, rope, 0.0)
    latent_ref[...] = total[3:CHUNKS]


def own_body(latent_ref, table_ref, query_ref, wk_ref, wv_ref, own_ref, fresh_ref):
    query = [query_ref[j].astype(BF16) for j in range(3)]
    pieces = [latent_ref[c, k] for c in range(2) for k in range(4)]
    squares = sum(jnp.sum(piece * piece, -1, keepdims=True) for piece in pieces)
    scale = lax.rsqrt(squares / (8 * LANES) + EPS)
    pieces = [p * scale * table_ref[LATENT_AT + k : LATENT_AT + k + 1] for k, p in enumerate(pieces)]
    for k, piece in enumerate(pieces):
        fresh_ref[k] = piece
    fresh = jnp.concatenate(pieces, 1)
    low = jnp.concatenate([fresh, jnp.zeros_like(fresh)], 0).astype(BF16)
    value = matmul(low, wv_ref[...])
    rope = table_ref[ROPE_AT : ROPE_AT + 4].astype(BF16).astype(F32)
    tiled = jnp.concatenate([rope, jnp.zeros_like(rope)], 0)
    key = keys_of(
        matmul(low, wk_ref[...]), tiled, table_ref[KN_AT : KN_AT + 1], table_ref[KR_AT : KR_AT + 1]
    )
    pad = jnp.zeros((LANES - 8, LANES), F32)
    key = [jnp.concatenate([k, pad], 0).astype(BF16) for k in key]
    value = [jnp.concatenate([v, pad], 0) for v in (value[:, :LANES], value[:, LANES:])]
    own = sum(matmul_t(q, k) for q, k in zip(query, key))
    for j, part in enumerate(attend([own], [value], [table_ref[SEEN_AT : SEEN_AT + 16] > 0.5])):
        own_ref[j] = part


def attend_body(table_ref, query_ref, *refs):
    block_refs, out_ref = refs[:-1], refs[-1]
    query = [query_ref[j].astype(BF16) for j in range(3)]
    anchor = table_ref[ANCHOR_AT : ANCHOR_AT + 1]
    nope_gain = table_ref[GAIN_AT : GAIN_AT + NOPE]
    rope_gain = table_ref[GAIN_AT + NOPE : GAIN_AT + QK]
    products, values, seen = [], [], []
    for k, block_ref in enumerate(block_refs):
        source = lax.rem(lax.axis_index("y") + SEQS - k, SEQS)
        start = (lax.axis_index("z") * SEQS + source) * LANES
        scales = [block_ref[SCALE_AT + h : SCALE_AT + h + 1] for h in range(HEADS)]
        rope = block_ref[TURN_AT : TURN_AT + ROPE]
        keys = [
            block_ref[NOPE * h : NOPE * h + NOPE] * scales[h] * nope_gain for h in range(HEADS)
        ] + [rope * scales[h] * rope_gain for h in range(HEADS)]
        key = jnp.concatenate(keys, 0).astype(BF16)
        products.append(sum(matmul(q, key[LANES * j : LANES * j + LANES]) for j, q in enumerate(query)))
        values.append([block_ref[VALUE_AT + LANES * j : VALUE_AT + LANES * j + LANES] for j in range(2)])
        seen.append((lanes_of((16, LANES)) + start).astype(F32) < anchor)
    packed = attend(products, values, seen)
    for k in range(out_ref.shape[0]):
        for j, part in enumerate(packed):
            out_ref[k, j] = part


def merge_body(in_ref, own_ref, fresh_ref, *refs):
    block_refs, out_ref = refs[:-1], refs[-1]
    y = lax.axis_index("y")
    share = lax.axis_index("x") * lax.axis_size("c") + lax.axis_index("c")
    parts = [[in_ref[k, j] for j in range(3)] for k in range(in_ref.shape[0])]
    parts.append([own_ref[j] for j in range(3)])
    peak = functools.reduce(jnp.maximum, [stats for _, _, stats in parts])
    first = second = total = 0.0
    for first_part, second_part, stats in parts:
        scale = jnp.exp(stats - peak)
        total = total + pltpu.roll(stats, LANES - HEADS, 1) * scale
        first = first + first_part * half_pick(scale[:, 0:1], scale[:, 1:2])
        second = second + second_part * half_pick(scale[:, 2:3], scale[:, 3:4])
    first = first / half_pick(total[:, 0:1], total[:, 1:2])
    second = second / half_pick(total[:, 2:3], total[:, 3:4])
    pad = jnp.zeros((4, LANES), F32)
    first = jnp.concatenate([first, pad], 0).astype(BF16)
    second = jnp.concatenate([second, pad], 0).astype(BF16)
    sums = [jnp.zeros((8, LANES), F32) for _ in range(SEQS)]
    for k, block_ref in enumerate(block_refs):
        weight = block_ref[WEIGHT_AT : WEIGHT_AT + LANES].astype(BF16)
        low = matmul_t(first, weight) + pltpu.roll(matmul_t(second, weight), NOPE, 1)
        both = half_pick(low, pltpu.roll(low, NOPE, 1))
        place = lax.rem(y + SEQS - k, SEQS)
        sums = [jnp.where(place == j, both, sums[j]) for j in range(SEQS)]
    packed = (half_pick(sums[0], sums[1])[0:4], half_pick(sums[2], sums[3])[0:4], fresh_ref[share])
    for k in range(out_ref.shape[0]):
        for j, part in enumerate(packed):
            out_ref[k, j] = part


def gather_body(whole_ref, own_ref, square_ref, latent_ref):
    y = lax.axis_index("y")
    size = whole_ref.shape[0]
    peers = size // SEQS
    in_ref = [whole_ref.at[(k - PLANE_FIRST) % size] for k in range(size)]
    lane = lanes_of((PROPS, LANES))
    squares = jnp.zeros((PROPS, LANES), F32)
    for s in range(SEQS):
        first, second = in_ref[peers * s][0], in_ref[peers * s][1]
        for t in range(1, peers):
            first = first + in_ref[peers * s + t][0]
            second = second + in_ref[peers * s + t][1]
        square = jnp.sum(first * first + second * second, -1, keepdims=True)
        squares = squares + jnp.where(lane == PROPS * s + rows_of(lane.shape), square, 0.0)
        picked = jnp.where(y < 2, first, second)
        own_ref[s] = jnp.where(lax.rem(y, 2) == 0, picked, pltpu.roll(picked, NOPE, 1))
        for t in range(peers):
            latent_ref[s, :, LANES * t : LANES * t + LANES] = in_ref[peers * s + t][2]
    squares = jnp.sum(squares, 0, keepdims=True)
    for k in range(square_ref.shape[0]):
        square_ref[k] = squares


def finish_body(in_ref, own_ref, table_ref, window_ref, fresh_ref, copy_hbm, mixed_hbm, out_hbm, patch_ref, mixed_ref, sems):
    del copy_hbm
    positions = out_hbm.shape[1]
    begun = table_ref[START_AT : START_AT + 1]
    lane = lanes_of(begun.shape)
    starts = [jnp.sum(jnp.where(lane == s, begun, 0.0)).astype(jnp.int32) for s in range(SEQS)]
    for s, start in enumerate(starts):

        @pl.when((start > -PROPS) & (start < positions))
        def _(s=s, start=start):
            base = window_base(start, positions)
            window = window_ref[s].astype(F32)
            row = rows_of(window.shape) + base
            for p in range(PROPS):
                window = jnp.where(row == start + p, fresh_ref[s, p : p + 1, :], window)
            patch_ref[s] = window.astype(BF16)
            pltpu.make_async_copy(patch_ref.at[s], out_hbm.at[s, pl.ds(base, WINDOW), :], sems.at[s]).start()

    total = in_ref[0]
    for k in range(1, in_ref.shape[0]):
        total = total + in_ref[k]
    gain = table_ref[OUT_AT : OUT_AT + 1, 0:NOPE]
    spread = (PROPS, LANES)
    for s in range(SEQS):
        square = jnp.where(lanes_of(spread) == PROPS * s + rows_of(spread), total, 0.0)
        scale = lax.rsqrt(jnp.sum(square, -1, keepdims=True) / D + EPS)
        mixed_ref[s] = (own_ref[s, :, :NOPE] * scale * gain).astype(BF16)
    leaving = pltpu.make_async_copy(mixed_ref, mixed_hbm, sems.at[SEQS])
    leaving.start()
    for s, start in enumerate(starts):

        @pl.when((start > -PROPS) & (start < positions))
        def _(s=s, start=start):
            base = window_base(start, positions)
            pltpu.make_async_copy(patch_ref.at[s], out_hbm.at[s, pl.ds(base, WINDOW), :], sems.at[s]).wait()

    leaving.wait()


def swap(parts, axis, first=0):
    groups = None
    if first:
        size = lax.axis_size(axis)
        groups = [[(first + k) % size for k in range(size)]]
    return lax.all_to_all(
        parts, axis, split_axis=0, concat_axis=0, tiled=True, axis_index_groups=groups
    )


def body(
    tokens,
    parents,
    lengths,
    accepted,
    in_gain,
    w_query,
    w_latent,
    w_rope_key,
    latent_gain,
    query_gain,
    key_gain,
    w_key_up,
    w_value_up,
    w_out,
    out_gain,
    cache_latent,
    cache_rope,
):
    depth, tall = lax.axis_size("z"), lax.axis_size("y")
    plane = lax.axis_size(PLANE)
    inverse = 10000.0 ** (-(np.arange(LANES) % 16).astype(np.float32) / 16)
    inverse = jnp.asarray(inverse.astype(np.float32).reshape(1, LANES))
    rope_cols = jnp.swapaxes(cache_rope, 1, 2)

    in_row = in_gain.reshape(1, -1)

    def from_hbm(body, outs, out_specs, args, extra):
        args = [pltpu.with_memory_space_constraint(a, pltpu.HBM) for a in args]
        scratch = [
            (pltpu.SMEM if a.dtype == jnp.int32 else pltpu.VMEM)(a.shape, a.dtype) for a in args
        ]
        return kernel(
            body,
            outs,
            *args,
            specs=[HBM] * len(args),
            out_specs=out_specs,
            scratch=[*scratch, *extra, pltpu.SemaphoreType.DMA((len(args) + 1,))],
            mebibytes=16,
        )

    sent, block_0, block_1, block_2, block_3 = from_hbm(
        start_body,
        [((tall, CHUNKS, PROPS, LANES), F32), *[((BLOCK_ROWS, LANES), F32)] * SEQS],
        [HBM] + [VMEM] * 4,
        (tokens, in_row, w_query, w_latent, w_out.T, rope_cols, w_key_up, w_value_up, cache_latent),
        [pltpu.VMEM((SEQS * cache_latent.shape[1], 256), F32)] * 2
        + [pltpu.VMEM((tall, CHUNKS, PROPS, LANES), F32)],
    )
    table, windows, new_rope, kept = from_hbm(
        aside_body,
        [((TABLE_ROWS, LANES), F32), ((SEQS, WINDOW, 1024), BF16), (rope_cols.shape, BF16), (cache_latent.shape, BF16)],
        [VMEM] * 3 + [HBM],
        (
            parents,
            lengths,
            accepted,
            tokens,
            in_row,
            w_rope_key.T,
            inverse,
            latent_gain.reshape(1, -1),
            query_gain.reshape(1, -1),
            key_gain.reshape(1, -1),
            out_gain.reshape(1, -1),
            rope_cols,
            cache_latent,
        ),
        [],
    )
    reduced = swap(sent, "y", TALL_FIRST)
    leaving = [block_1, block_2, block_3]
    moved = {0: block_0}
    for k in (2, 1, 3):
        moved[k] = lax.ppermute(leaving[k - 1], "y", [(i, (i + k) % SEQS) for i in range(SEQS)])
    blocks = [moved[k] for k in range(SEQS)]
    spread = kernel(relay_body, [((depth, CHUNKS, PROPS, LANES), F32)], reduced)
    gathered = swap(spread, "z", depth // 2)
    query, latent_half = kernel(query_body, [((3, 16, LANES), F32), ((4, PROPS, LANES), F32)], gathered, table)
    latent_both = lax.all_gather(latent_half, "c")
    own, fresh = kernel(
        own_body, [((3, PROPS, LANES), F32), ((8, PROPS, LANES), F32)], latent_both, table, query, w_key_up, w_value_up
    )
    partial = kernel(attend_body, [((depth, 3, PROPS, LANES), F32)], table, query, *blocks)
    partials = swap(partial, "z", depth // 2)
    projected = kernel(merge_body, [((plane, 3, PROPS, LANES), F32)], partials, own, fresh, *blocks)
    projections = swap(projected, PLANE, PLANE_FIRST)
    own_columns, squares, fresh_all = kernel(
        gather_body, [((SEQS, PROPS, LANES), F32), ((depth, 1, LANES), F32), ((SEQS, PROPS, 1024), F32)], projections
    )
    square_parts = swap(squares, "z", depth // 2)
    mixed, new_latent = kernel(
        finish_body,
        [((SEQS, PROPS, NOPE), BF16), (cache_latent.shape, BF16)],
        square_parts,
        own_columns,
        table,
        windows,
        fresh_all,
        kept,
        specs=[VMEM] * 5 + [HBM],
        out_specs=[HBM, HBM],
        scratch=[
            pltpu.VMEM((SEQS, WINDOW, 1024), BF16),
            pltpu.VMEM((SEQS, PROPS, NOPE), BF16),
            pltpu.SemaphoreType.DMA((SEQS + 1,)),
        ],
        aliases={5: 1},
    )
    return (mixed, new_latent, jnp.swapaxes(new_rope, 1, 2))


def solution(mesh):
    kv, tp = mesh.shape["kv"], mesh.shape["tp"]
    finer = Mesh(mesh.devices.reshape(kv // 4, 4, tp // 2, 2), ("z", "y", "x", "c"))
    tp_axes = ("x", "c")
    placed = (
        P(),
        P(),
        P(),
        P(),
        P(),
        P(KV, tp_axes),
        P(KV, None),
        P(),
        P(),
        P(),
        P(),
        P(None, tp_axes),
        P(None, tp_axes),
        P(tp_axes, KV),
        P(KV),
        P(None, KV, None),
        P(None, KV, None),
    )
    return jax.shard_map(
        body,
        mesh=finer,
        in_specs=placed,
        out_specs=(P(None, None, KV), P(None, KV, None), P(None, KV, None)),
        check_vma=False,
    )
```

```python
import functools

import jax
import jax.numpy as jnp
import numpy as np
from jax import lax
from jax.experimental import pallas as pl
from jax.experimental.pallas import tpu as pltpu
from jax.sharding import Mesh
from jax.sharding import PartitionSpec as P


D = 4096
NOPE = 64
ROPE = 32
QK = 96
SEQS = 4
PROPS = 4
HEADS = 4
LANES = 128
EPS = 1e-06
KV = ("z", "y")
PLANE = ("y", "x", "c")
F32 = jnp.float32
BF16 = jnp.bfloat16
HIDDEN = -1e30

VMEM = pl.BlockSpec(memory_space=pltpu.VMEM)
HBM = pl.BlockSpec(memory_space=pltpu.HBM)
CHUNKS = 7
PLANE_FIRST, TALL_FIRST = 21, 2
TURN_AT, SCALE_AT, VALUE_AT, WEIGHT_AT, BLOCK_ROWS = 256, 288, 296, 552, 680
ROPE_AT, COS_AT, A_AT, B_AT, SEEN_AT, ANCHOR_AT = 0, 4, 8, 12, 16, 32
QN_AT, QR_AT, KN_AT, KR_AT, OUT_AT, START_AT, LATENT_AT = 33, 34, 35, 36, 37, 38, 40
GAIN_AT, TABLE_ROWS = 48, 144
WINDOW = 32


def kernel(body, outs, *args, specs=None, out_specs=None, scratch=(), aliases=None, mebibytes=8):
    shapes = [jax.ShapeDtypeStruct(shape, kind) for shape, kind in outs]
    out_specs = list(out_specs) if out_specs else [VMEM] * len(shapes)
    single = len(shapes) == 1
    return pl.pallas_call(
        body,
        out_shape=shapes[0] if single else shapes,
        in_specs=list(specs) if specs else [VMEM] * len(args),
        out_specs=out_specs[0] if single else out_specs,
        scratch_shapes=list(scratch),
        input_output_aliases=aliases or {},
        cost_estimate=pl.CostEstimate(flops=2_000_000, bytes_accessed=1_000_000, transcendentals=0),
        compiler_params=pltpu.CompilerParams(vmem_limit_bytes=mebibytes * 2**20),
    )(*args)


def lanes_of(shape):
    return lax.broadcasted_iota(jnp.int32, shape, len(shape) - 1)


def rows_of(shape):
    return lax.broadcasted_iota(jnp.int32, shape, len(shape) - 2)


def matmul(left, right):
    return lax.dot_general(left, right, (((1,), (0,)), ((), ())), preferred_element_type=F32)


def matmul_t(left, right):
    return lax.dot_general(left, right, (((1,), (1,)), ((), ())), preferred_element_type=F32)


def half_pick(low, high):
    shape = jnp.broadcast_shapes(low.shape, high.shape)
    shape = (*shape[:-1], LANES)
    return jnp.where(lanes_of(shape) < NOPE, low, high)


def quarter_pick(parts):
    shape = (*parts[0].shape[:-1], LANES)
    lane = lanes_of(shape)
    return jnp.where(
        lane < NOPE,
        jnp.where(lane < ROPE, parts[0], parts[1]),
        jnp.where(lane < NOPE + ROPE, parts[2], parts[3]),
    )


def head_scales(first, second, rope_squares):
    lane = lanes_of(first.shape)
    found = []
    for h, part in enumerate((first, first, second, second)):
        inside = lane < NOPE if h % 2 == 0 else lane >= NOPE
        squares = jnp.sum(jnp.where(inside, part * part, 0.0), -1, keepdims=True)
        found.append(lax.rsqrt((squares + rope_squares[h]) / QK + EPS))
    return found


def gains(gain_row):
    nope = gain_row[:, :NOPE]
    rope = gain_row[:, NOPE:QK]
    return jnp.concatenate([nope, nope], 1), jnp.concatenate([rope] * 4, 1)


def keys_of(nope, rope_tiled, nope_gain, rope_gain):
    first, second = nope[:, :LANES], nope[:, LANES:]
    lane = lanes_of(rope_tiled.shape)
    rope_sum = jnp.sum(jnp.where(lane < ROPE, rope_tiled * rope_tiled, 0.0), -1, keepdims=True)
    scales = head_scales(first, second, [rope_sum] * 4)
    return (
        first * half_pick(scales[0], scales[1]) * nope_gain,
        second * half_pick(scales[2], scales[3]) * nope_gain,
        rope_tiled * quarter_pick(scales) * rope_gain,
    )


def attend(products, values, seen):
    scale = QK ** (-0.5)
    scores = [jnp.where(v, p * scale, HIDDEN) for p, v in zip(products, seen)]
    peak = functools.reduce(jnp.maximum, [jnp.max(s, -1, keepdims=True) for s in scores])
    weights = [jnp.where(v, jnp.exp(s - peak), 0.0) for s, v in zip(scores, seen)]
    total = sum(jnp.sum(w, -1, keepdims=True) for w in weights)
    sums = [0.0, 0.0]
    for weight, value in zip(weights, values):
        low = weight.astype(BF16)
        for j, part in enumerate(value):
            high_part = part.astype(BF16)
            rest = (part - high_part.astype(F32)).astype(BF16)
            sums[j] = sums[j] + matmul(low, high_part) + matmul(low, rest)
    first = half_pick(sums[0][0:4], sums[0][4:8])
    second = half_pick(sums[1][8:12], sums[1][12:16])
    lane = lanes_of((PROPS, LANES))
    stats = jnp.zeros((PROPS, LANES), F32)
    for h in range(HEADS):
        stats = jnp.where(lane == h, peak[4 * h : 4 * h + 4], stats)
        stats = jnp.where(lane == HEADS + h, total[4 * h : 4 * h + 4], stats)
    return first, second, stats


def sine_cosine(angle):
    turns = jnp.floor(angle * (2.0 / np.pi) + 0.5)
    rest = ((angle - turns * 1.5703125) - turns * 4.837512969970703125e-4) - turns * 7.549789954891882e-8
    square = rest * rest
    sine = rest + rest * square * (
        -1.6666654611e-1 + square * (8.3321608736e-3 + square * -1.9515295891e-4)
    )
    cosine = (
        1.0
        - 0.5 * square
        + square
        * square
        * (4.166664568298827e-2 + square * (-1.388731625493765e-3 + square * 2.443315711809948e-5))
    )
    quadrant = turns - 4.0 * jnp.floor(turns * 0.25)
    odd = (quadrant == 1.0) | (quadrant == 3.0)
    sine_out = jnp.where(odd, cosine, sine)
    cosine_out = jnp.where(odd, sine, cosine)
    sine_out = jnp.where(quadrant >= 2.0, -sine_out, sine_out)
    cosine_out = jnp.where((quadrant == 1.0) | (quadrant == 2.0), -cosine_out, cosine_out)
    return sine_out, cosine_out


def turn(rope_tiled, cosine, sine_a, sine_b):
    return (
        rope_tiled * cosine
        + pltpu.roll(rope_tiled, LANES - 16, 1) * sine_a
        + pltpu.roll(rope_tiled, 16, 1) * sine_b
    )


def ancestors(parents_ref, s):
    masks = []
    for i in range(PROPS):
        mask = jnp.int32(1 << i)
        if i:
            parent = parents_ref[s, i]
            for j in range(i):
                mask = mask + jnp.where(parent == j, masks[j], 0)
        masks.append(mask)
    return masks


def bits(mask):
    return sum((mask >> j) & 1 for j in range(PROPS))


def load(sources, targets, sems):
    copies = [pltpu.make_async_copy(a, b, sems.at[k]) for k, (a, b) in enumerate(zip(sources, targets))]
    for copy in copies:
        copy.start()
    return copies


def start_body(*refs):
    sources, refs = refs[:9], refs[9:]
    (out_hbm, *block_refs), refs = refs[:5], refs[5:]
    targets, (nope_ref, value_ref, out_ref, sems) = refs[:9], refs[9:]
    tok_ref, gain_ref, wq_ref, wl_ref, wo_ref, rope_ref, wk_ref, wv_ref, cache_ref = targets
    copies = load(sources, targets, sems)
    for copy in copies[:4]:
        copy.wait()
    y = lax.axis_index("y")
    kv = lax.axis_index("z") * lax.axis_size("y") + y
    rows = wq_ref.shape[0]
    width = max(rows, LANES)
    per = width // rows
    base = pl.multiple_of((kv // per) * width, LANES)
    positions = cache_ref.shape[1]

    parts = []
    for s in range(SEQS):
        tok = tok_ref[s].astype(F32)
        scale = lax.rsqrt(jnp.sum(tok * tok, -1, keepdims=True) / D + EPS)
        piece = tok_ref[s, :, pl.ds(base, width)].astype(F32)
        parts.append(piece * scale * gain_ref[:, pl.ds(base, width)])
    part = jnp.concatenate(parts, 0)
    if per > 1:
        part = jnp.where(lanes_of(part.shape) // rows == kv % per, part, 0.0)
    part = part.astype(BF16)
    half = wl_ref.shape[1] // 2
    wl = wl_ref[:, pl.ds(pl.multiple_of(lax.axis_index("c") * half, LANES), half)]
    query = matmul(part, jnp.concatenate([wq_ref[...]] * per, 0))
    latent = matmul(part, jnp.concatenate([wl] * per, 0))
    nope = [query[:, QK * h : QK * h + NOPE] for h in range(HEADS)]
    rope = [query[:, QK * h + NOPE : QK * h + QK] for h in range(HEADS)]
    chunks = [
        jnp.concatenate(nope[:2], 1),
        jnp.concatenate(nope[2:], 1),
        jnp.concatenate(rope, 1),
    ] + [latent[:, LANES * k : LANES * k + LANES] for k in range(half // LANES)]
    for s in range(SEQS):
        for k, chunk in enumerate(chunks):
            out_ref[(s - TALL_FIRST) % SEQS, k] = chunk[4 * s : 4 * s + 4]
    leaving = pltpu.make_async_copy(out_ref, out_hbm, sems.at[len(copies)])
    leaving.start()

    for copy in copies[4:]:
        copy.wait()
    whole = cache_ref[...].reshape(SEQS * positions, cache_ref.shape[2])
    nope_ref[...] = matmul(whole, wk_ref[...])
    value_ref[...] = matmul(whole, wv_ref[...])
    weights = wo_ref[...].astype(F32)
    for k, block_ref in enumerate(block_refs):
        s = lax.rem(y + k, SEQS)
        at = pl.ds(pl.multiple_of(s * positions, positions), positions)
        old = rope_ref[s].astype(F32)
        old_sum = jnp.sum(old * old, 0, keepdims=True)
        block_ref[TURN_AT : TURN_AT + ROPE] = old
        for j in range(2):
            lanes = slice(LANES * j, LANES * j + LANES)
            flat = nope_ref[at, lanes].T
            block_ref[lanes] = flat
            block_ref[VALUE_AT + LANES * j : VALUE_AT + LANES * j + LANES] = value_ref[at, lanes]
            for i in range(2):
                dims = flat[NOPE * i : NOPE * i + NOPE]
                squares = jnp.sum(dims * dims, 0, keepdims=True) + old_sum
                h = SCALE_AT + 2 * j + i
                block_ref[h : h + 1] = lax.rsqrt(squares / QK + EPS)
        block_ref[SCALE_AT + 4 : SCALE_AT + 8] = jnp.zeros((4, LANES), F32)
        block_ref[WEIGHT_AT : WEIGHT_AT + 64] = weights[:, :LANES]
        block_ref[WEIGHT_AT + 64 : WEIGHT_AT + 128] = weights[:, LANES:]
    leaving.wait()


def aside_body(*refs):
    sources, refs = refs[:13], refs[13:]
    (table_ref, window_ref, rope_out_ref, copy_hbm), refs = refs[:4], refs[4:]
    targets, sems = refs[:13], refs[13]
    (
        parents_ref, lengths_ref, accepted_ref, tok_ref, gain_ref, wr_ref,
        inverse_ref, lgain_ref, qgain_ref, kgain_ref, ogain_ref, rope_ref, cache_ref,
    ) = targets
    copies = load(sources, targets, sems)
    for copy in copies:
        copy.wait()
    kept = pltpu.make_async_copy(cache_ref, copy_hbm, sems.at[len(copies)])
    kept.start()
    y = lax.axis_index("y")
    kv = lax.axis_index("z") * lax.axis_size("y") + y
    positions = cache_ref.shape[1]
    normed = []
    for s in range(SEQS):
        tok = tok_ref[s].astype(F32)
        scale = lax.rsqrt(jnp.sum(tok * tok, -1, keepdims=True) / D + EPS)
        normed.append(tok * scale * gain_ref[...])

    row = rows_of((16, LANES))
    place = jnp.zeros((16, LANES), F32)
    starts = []
    for s in range(SEQS):
        anchor = lengths_ref[s] + accepted_ref[s]
        starts.append(anchor - kv * positions)
        for i, mask in enumerate(ancestors(parents_ref, s)):
            place = jnp.where(row == 4 * s + i, (anchor + bits(mask) - 1).astype(F32), place)
    raw = matmul_t(jnp.concatenate(normed, 0).astype(BF16), wr_ref[...])
    raw = jnp.concatenate([raw] * 4, 1)
    sine, cosine = sine_cosine(place * inverse_ref[...])
    early = lanes_of((16, LANES)) % ROPE < 16
    sine_a = jnp.where(early, -sine, 0.0)
    sine_b = jnp.where(early, 0.0, sine)
    fresh = turn(raw, cosine, sine_a, sine_b)
    for at, full in ((ROPE_AT, fresh), (COS_AT, cosine), (A_AT, sine_a), (B_AT, sine_b)):
        own = full[0:4]
        for s in range(1, SEQS):
            own = jnp.where(y == s, full[4 * s : 4 * s + 4], own)
        table_ref[at : at + 4] = own
    masks = ancestors(parents_ref, y)
    prop, lane = row % PROPS, lanes_of((16, LANES))
    seen = jnp.zeros((16, LANES), jnp.int32)
    for i in range(PROPS):
        for j in range(i + 1):
            seen = jnp.where((prop == i) & (lane == j), (masks[i] >> j) & 1, seen)
    table_ref[SEEN_AT : SEEN_AT + 16] = seen.astype(F32)
    anchor = (lengths_ref[y] + accepted_ref[y]).astype(F32)
    table_ref[ANCHOR_AT : ANCHOR_AT + 1] = jnp.zeros((1, LANES), F32) + anchor
    nope_gain, rope_gain = gains(kgain_ref[...])
    table_ref[KN_AT : KN_AT + 1], table_ref[KR_AT : KR_AT + 1] = nope_gain, rope_gain
    table_ref[QN_AT : QN_AT + 1], table_ref[QR_AT : QR_AT + 1] = gains(qgain_ref[...])
    table_ref[OUT_AT : OUT_AT + 1] = jnp.concatenate([ogain_ref[...]] * (LANES // ogain_ref.shape[1]), 1)
    spot = lanes_of((2, LANES))
    begun = jnp.zeros((2, LANES), F32)
    for s in range(SEQS):
        begun = jnp.where(spot == s, starts[s].astype(F32), begun)
    table_ref[START_AT : START_AT + 2] = begun
    for k in range(8):
        table_ref[LATENT_AT + k : LATENT_AT + k + 1] = lgain_ref[:, LANES * k : LANES * k + LANES]
    tall_gain = jnp.concatenate([nope_gain, rope_gain, jnp.zeros((6, LANES), F32)], 0)
    tall_gain = jnp.concatenate([tall_gain] * (LANES // 8), 0).T
    table_ref[GAIN_AT : GAIN_AT + NOPE] = jnp.zeros((NOPE, LANES), F32) + tall_gain[:NOPE, 0:1]
    table_ref[GAIN_AT + NOPE : GAIN_AT + QK] = jnp.zeros((ROPE, LANES), F32) + tall_gain[:ROPE, 1:2]
    flipped = jnp.concatenate([fresh, jnp.zeros((LANES - 16, LANES), F32)], 0).T[:ROPE]

    for s in range(SEQS):
        old = rope_ref[s].astype(F32)
        spot = lanes_of(old.shape)
        for p in range(PROPS):
            old = jnp.where(spot == starts[s] + p, flipped[:, 4 * s + p : 4 * s + p + 1], old)
        rope_out_ref[s] = old.astype(BF16)
        window_ref[s] = cache_ref[s, pl.ds(window_base(starts[s], positions), WINDOW), :]
    kept.wait()


def window_base(start, positions):
    return pl.multiple_of(jnp.clip(start // 16, 0, positions // 16 - WINDOW // 16) * 16, 16)


def relay_body(in_ref, out_ref):
    total = in_ref[0]
    for k in range(1, in_ref.shape[0]):
        total = total + in_ref[k]
    for k in range(out_ref.shape[0]):
        out_ref[k] = total


def query_body(in_ref, table_ref, query_ref, latent_ref):
    total = in_ref[0]
    for k in range(1, in_ref.shape[0]):
        total = total + in_ref[k]
    first, second = total[0], total[1]
    rope = turn(
        total[2],
        table_ref[COS_AT : COS_AT + 4],
        table_ref[A_AT : A_AT + 4],
        table_ref[B_AT : B_AT + 4],
    )
    lane = lanes_of(rope.shape)
    sums = [
        jnp.sum(jnp.where(lane // ROPE == h, rope * rope, 0.0), -1, keepdims=True)
        for h in range(HEADS)
    ]
    scales = head_scales(first, second, sums)
    nope_gain, rope_gain = table_ref[QN_AT : QN_AT + 1], table_ref[QR_AT : QR_AT + 1]
    first = first * half_pick(scales[0], scales[1]) * nope_gain
    second = second * half_pick(scales[2], scales[3]) * nope_gain
    rope = rope * quarter_pick(scales) * rope_gain
    for h in range(HEADS):
        inside = (lane < NOPE) if h % 2 == 0 else (lane >= NOPE)
        empty = jnp.zeros_like(first)
        query_ref[0, 4 * h : 4 * h + 4] = jnp.where(inside, first, 0.0) if h < 2 else empty
        query_ref[1, 4 * h : 4 * h + 4] = jnp.where(inside, second, 0.0) if h >= 2 else empty
        query_ref[2, 4 * h : 4 * h + 4] = jnp.where(lane // ROPE == h, rope, 0.0)
    latent_ref[...] = total[3:CHUNKS]


def own_body(latent_ref, table_ref, query_ref, wk_ref, wv_ref, own_ref, fresh_ref):
    query = [query_ref[j].astype(BF16) for j in range(3)]
    pieces = [latent_ref[c, k] for c in range(2) for k in range(4)]
    squares = sum(jnp.sum(piece * piece, -1, keepdims=True) for piece in pieces)
    scale = lax.rsqrt(squares / (8 * LANES) + EPS)
    pieces = [p * scale * table_ref[LATENT_AT + k : LATENT_AT + k + 1] for k, p in enumerate(pieces)]
    for k, piece in enumerate(pieces):
        fresh_ref[k] = piece
    fresh = jnp.concatenate(pieces, 1)
    low = jnp.concatenate([fresh, jnp.zeros_like(fresh)], 0).astype(BF16)
    value = matmul(low, wv_ref[...])
    rope = table_ref[ROPE_AT : ROPE_AT + 4].astype(BF16).astype(F32)
    tiled = jnp.concatenate([rope, jnp.zeros_like(rope)], 0)
    key = keys_of(
        matmul(low, wk_ref[...]), tiled, table_ref[KN_AT : KN_AT + 1], table_ref[KR_AT : KR_AT + 1]
    )
    pad = jnp.zeros((LANES - 8, LANES), F32)
    key = [jnp.concatenate([k, pad], 0).astype(BF16) for k in key]
    value = [jnp.concatenate([v, pad], 0) for v in (value[:, :LANES], value[:, LANES:])]
    own = sum(matmul_t(q, k) for q, k in zip(query, key))
    for j, part in enumerate(attend([own], [value], [table_ref[SEEN_AT : SEEN_AT + 16] > 0.5])):
        own_ref[j] = part


def attend_body(table_ref, query_ref, *refs):
    block_refs, out_ref = refs[:-1], refs[-1]
    query = [query_ref[j].astype(BF16) for j in range(3)]
    anchor = table_ref[ANCHOR_AT : ANCHOR_AT + 1]
    nope_gain = table_ref[GAIN_AT : GAIN_AT + NOPE]
    rope_gain = table_ref[GAIN_AT + NOPE : GAIN_AT + QK]
    products, values, seen = [], [], []
    for k, block_ref in enumerate(block_refs):
        source = lax.rem(lax.axis_index("y") + SEQS - k, SEQS)
        start = (lax.axis_index("z") * SEQS + source) * LANES
        scales = [block_ref[SCALE_AT + h : SCALE_AT + h + 1] for h in range(HEADS)]
        rope = block_ref[TURN_AT : TURN_AT + ROPE]
        keys = [
            block_ref[NOPE * h : NOPE * h + NOPE] * scales[h] * nope_gain for h in range(HEADS)
        ] + [rope * scales[h] * rope_gain for h in range(HEADS)]
        key = jnp.concatenate(keys, 0).astype(BF16)
        products.append(sum(matmul(q, key[LANES * j : LANES * j + LANES]) for j, q in enumerate(query)))
        values.append([block_ref[VALUE_AT + LANES * j : VALUE_AT + LANES * j + LANES] for j in range(2)])
        seen.append((lanes_of((16, LANES)) + start).astype(F32) < anchor)
    packed = attend(products, values, seen)
    for k in range(out_ref.shape[0]):
        for j, part in enumerate(packed):
            out_ref[k, j] = part


def merge_body(in_ref, own_ref, fresh_ref, *refs):
    block_refs, out_ref = refs[:-1], refs[-1]
    y = lax.axis_index("y")
    share = lax.axis_index("x") * lax.axis_size("c") + lax.axis_index("c")
    parts = [[in_ref[k, j] for j in range(3)] for k in range(in_ref.shape[0])]
    parts.append([own_ref[j] for j in range(3)])
    peak = functools.reduce(jnp.maximum, [stats for _, _, stats in parts])
    first = second = total = 0.0
    for first_part, second_part, stats in parts:
        scale = jnp.exp(stats - peak)
        total = total + pltpu.roll(stats, LANES - HEADS, 1) * scale
        first = first + first_part * half_pick(scale[:, 0:1], scale[:, 1:2])
        second = second + second_part * half_pick(scale[:, 2:3], scale[:, 3:4])
    first = first / half_pick(total[:, 0:1], total[:, 1:2])
    second = second / half_pick(total[:, 2:3], total[:, 3:4])
    pad = jnp.zeros((4, LANES), F32)
    first = jnp.concatenate([first, pad], 0).astype(BF16)
    second = jnp.concatenate([second, pad], 0).astype(BF16)
    sums = [jnp.zeros((8, LANES), F32) for _ in range(SEQS)]
    for k, block_ref in enumerate(block_refs):
        weight = block_ref[WEIGHT_AT : WEIGHT_AT + LANES].astype(BF16)
        low = matmul_t(first, weight) + pltpu.roll(matmul_t(second, weight), NOPE, 1)
        both = half_pick(low, pltpu.roll(low, NOPE, 1))
        place = lax.rem(y + SEQS - k, SEQS)
        sums = [jnp.where(place == j, both, sums[j]) for j in range(SEQS)]
    packed = (half_pick(sums[0], sums[1])[0:4], half_pick(sums[2], sums[3])[0:4], fresh_ref[share])
    for k in range(out_ref.shape[0]):
        for j, part in enumerate(packed):
            out_ref[k, j] = part


def gather_body(whole_ref, own_ref, square_ref, latent_ref):
    y = lax.axis_index("y")
    size = whole_ref.shape[0]
    peers = size // SEQS
    in_ref = [whole_ref.at[(k - PLANE_FIRST) % size] for k in range(size)]
    lane = lanes_of((PROPS, LANES))
    squares = jnp.zeros((PROPS, LANES), F32)
    for s in range(SEQS):
        first, second = in_ref[peers * s][0], in_ref[peers * s][1]
        for t in range(1, peers):
            first = first + in_ref[peers * s + t][0]
            second = second + in_ref[peers * s + t][1]
        square = jnp.sum(first * first + second * second, -1, keepdims=True)
        squares = squares + jnp.where(lane == PROPS * s + rows_of(lane.shape), square, 0.0)
        picked = jnp.where(y < 2, first, second)
        own_ref[s] = jnp.where(lax.rem(y, 2) == 0, picked, pltpu.roll(picked, NOPE, 1))
        for t in range(peers):
            latent_ref[s, :, LANES * t : LANES * t + LANES] = in_ref[peers * s + t][2]
    squares = jnp.sum(squares, 0, keepdims=True)
    for k in range(square_ref.shape[0]):
        square_ref[k] = squares


def finish_body(in_ref, own_ref, table_ref, window_ref, fresh_ref, copy_hbm, mixed_hbm, out_hbm, patch_ref, mixed_ref, sems):
    del copy_hbm
    positions = out_hbm.shape[1]
    begun = table_ref[START_AT : START_AT + 1]
    lane = lanes_of(begun.shape)
    starts = [jnp.sum(jnp.where(lane == s, begun, 0.0)).astype(jnp.int32) for s in range(SEQS)]
    for s, start in enumerate(starts):

        @pl.when((start > -PROPS) & (start < positions))
        def _(s=s, start=start):
            base = window_base(start, positions)
            window = window_ref[s].astype(F32)
            row = rows_of(window.shape) + base
            for p in range(PROPS):
                window = jnp.where(row == start + p, fresh_ref[s, p : p + 1, :], window)
            patch_ref[s] = window.astype(BF16)
            pltpu.make_async_copy(patch_ref.at[s], out_hbm.at[s, pl.ds(base, WINDOW), :], sems.at[s]).start()

    total = in_ref[0]
    for k in range(1, in_ref.shape[0]):
        total = total + in_ref[k]
    gain = table_ref[OUT_AT : OUT_AT + 1, 0:NOPE]
    spread = (PROPS, LANES)
    for s in range(SEQS):
        square = jnp.where(lanes_of(spread) == PROPS * s + rows_of(spread), total, 0.0)
        scale = lax.rsqrt(jnp.sum(square, -1, keepdims=True) / D + EPS)
        mixed_ref[s] = (own_ref[s, :, :NOPE] * scale * gain).astype(BF16)
    leaving = pltpu.make_async_copy(mixed_ref, mixed_hbm, sems.at[SEQS])
    leaving.start()
    for s, start in enumerate(starts):

        @pl.when((start > -PROPS) & (start < positions))
        def _(s=s, start=start):
            base = window_base(start, positions)
            pltpu.make_async_copy(patch_ref.at[s], out_hbm.at[s, pl.ds(base, WINDOW), :], sems.at[s]).wait()

    leaving.wait()


def swap(parts, axis, first=0, apart=False):
    groups = None
    if first:
        size = lax.axis_size(axis)
        order = range(size)
        if apart:
            order = [k // 2 + (k % 2) * (size // 2) for k in range(size)]
        groups = [[(first + k) % size for k in order]]
    return lax.all_to_all(
        parts, axis, split_axis=0, concat_axis=0, tiled=True, axis_index_groups=groups
    )


def body(
    tokens,
    parents,
    lengths,
    accepted,
    in_gain,
    w_query,
    w_latent,
    w_rope_key,
    latent_gain,
    query_gain,
    key_gain,
    w_key_up,
    w_value_up,
    w_out,
    out_gain,
    cache_latent,
    cache_rope,
):
    depth, tall = lax.axis_size("z"), lax.axis_size("y")
    plane = lax.axis_size(PLANE)
    inverse = 10000.0 ** (-(np.arange(LANES) % 16).astype(np.float32) / 16)
    inverse = jnp.asarray(inverse.astype(np.float32).reshape(1, LANES))
    rope_cols = jnp.swapaxes(cache_rope, 1, 2)

    in_row = in_gain.reshape(1, -1)

    def from_hbm(body, outs, out_specs, args, extra):
        args = [pltpu.with_memory_space_constraint(a, pltpu.HBM) for a in args]
        scratch = [
            (pltpu.SMEM if a.dtype == jnp.int32 else pltpu.VMEM)(a.shape, a.dtype) for a in args
        ]
        return kernel(
            body,
            outs,
            *args,
            specs=[HBM] * len(args),
            out_specs=out_specs,
            scratch=[*scratch, *extra, pltpu.SemaphoreType.DMA((len(args) + 1,))],
            mebibytes=16,
        )

    sent, block_0, block_1, block_2, block_3 = from_hbm(
        start_body,
        [((tall, CHUNKS, PROPS, LANES), F32), *[((BLOCK_ROWS, LANES), F32)] * SEQS],
        [HBM] + [VMEM] * 4,
        (tokens, in_row, w_query, w_latent, w_out.T, rope_cols, w_key_up, w_value_up, cache_latent),
        [pltpu.VMEM((SEQS * cache_latent.shape[1], 256), F32)] * 2
        + [pltpu.VMEM((tall, CHUNKS, PROPS, LANES), F32)],
    )
    table, windows, new_rope, kept = from_hbm(
        aside_body,
        [((TABLE_ROWS, LANES), F32), ((SEQS, WINDOW, 1024), BF16), (rope_cols.shape, BF16), (cache_latent.shape, BF16)],
        [VMEM] * 3 + [HBM],
        (
            parents,
            lengths,
            accepted,
            tokens,
            in_row,
            w_rope_key.T,
            inverse,
            latent_gain.reshape(1, -1),
            query_gain.reshape(1, -1),
            key_gain.reshape(1, -1),
            out_gain.reshape(1, -1),
            rope_cols,
            cache_latent,
        ),
        [],
    )
    reduced = swap(sent, "y", TALL_FIRST)
    leaving = [block_1, block_2, block_3]
    moved = {0: block_0}
    for k in (2, 1, 3):
        moved[k] = lax.ppermute(leaving[k - 1], "y", [(i, (i + k) % SEQS) for i in range(SEQS)])
    blocks = [moved[k] for k in range(SEQS)]
    spread = kernel(relay_body, [((depth, CHUNKS, PROPS, LANES), F32)], reduced)
    gathered = swap(spread, "z", depth // 2 + 1)
    query, latent_half = kernel(query_body, [((3, 16, LANES), F32), ((4, PROPS, LANES), F32)], gathered, table)
    latent_both = lax.all_gather(latent_half, "c")
    own, fresh = kernel(
        own_body, [((3, PROPS, LANES), F32), ((8, PROPS, LANES), F32)], latent_both, table, query, w_key_up, w_value_up
    )
    partial = kernel(attend_body, [((depth, 3, PROPS, LANES), F32)], table, query, *blocks)
    partials = swap(partial, "z", depth // 2 + 1, apart=True)
    projected = kernel(merge_body, [((plane, 3, PROPS, LANES), F32)], partials, own, fresh, *blocks)
    projections = swap(projected, PLANE, PLANE_FIRST)
    own_columns, squares, fresh_all = kernel(
        gather_body, [((SEQS, PROPS, LANES), F32), ((depth, 1, LANES), F32), ((SEQS, PROPS, 1024), F32)], projections
    )
    square_parts = swap(squares, "z", depth // 2 + 1)
    mixed, new_latent = kernel(
        finish_body,
        [((SEQS, PROPS, NOPE), BF16), (cache_latent.shape, BF16)],
        square_parts,
        own_columns,
        table,
        windows,
        fresh_all,
        kept,
        specs=[VMEM] * 5 + [HBM],
        out_specs=[HBM, HBM],
        scratch=[
            pltpu.VMEM((SEQS, WINDOW, 1024), BF16),
            pltpu.VMEM((SEQS, PROPS, NOPE), BF16),
            pltpu.SemaphoreType.DMA((SEQS + 1,)),
        ],
        aliases={5: 1},
    )
    return (mixed, new_latent, jnp.swapaxes(new_rope, 1, 2))


def solution(mesh):
    kv, tp = mesh.shape["kv"], mesh.shape["tp"]
    finer = Mesh(mesh.devices.reshape(kv // 4, 4, tp // 2, 2), ("z", "y", "x", "c"))
    tp_axes = ("x", "c")
    placed = (
        P(),
        P(),
        P(),
        P(),
        P(),
        P(KV, tp_axes),
        P(KV, None),
        P(),
        P(),
        P(),
        P(),
        P(None, tp_axes),
        P(None, tp_axes),
        P(tp_axes, KV),
        P(KV),
        P(None, KV, None),
        P(None, KV, None),
    )
    return jax.shard_map(
        body,
        mesh=finer,
        in_specs=placed,
        out_specs=(P(None, None, KV), P(None, KV, None), P(None, KV, None)),
        check_vma=False,
    )
```
